512 devices in a mesh: sp: 128 (over z, x, core), tp: 4 (over y).
Axes of the slice: x: 4, y: 4, z: 16, core: 2. Of those that a mesh axis runs over, the one named last changes fastest.
Arguments:
- tokens: bfloat16 [65536, 2048], P('sp', 'tp'), may hold values from -72 to 72
- w_query: bfloat16 [2048, 1024], P('sp', 'tp'), may hold values from -0.125 to 0.125
- w_key: bfloat16 [2048, 256], P('sp', 'tp'), may hold values from -0.125 to 0.125
- w_value: bfloat16 [2048, 256], P('sp', 'tp'), may hold values from -0.125 to 0.125
- w_pool_in: bfloat16 [2048, 1024], P('sp', 'tp'), may hold values from -0.125 to 0.125
- sink: float32 [16], P('tp'), may hold values from 3 to 7
- w_pool: bfloat16 [4, 256, 256], P('tp'), may hold values from -0.375 to 0.375
- pool_scale: float32 [1024], P('tp'), may hold values from 0.1 to 1.9
- w_out_attn: bfloat16 [1024, 2048], P('tp', 'sp'), may hold values from -0.5 to 0.5
- w_out_pool: bfloat16 [1024, 2048], P('tp', 'sp'), may hold values from -0.125 to 0.125
- out_gain: float32 [2048], P('tp'), may hold values from 0.1 to 1.9
Outputs:
- mixed: bfloat16 [65536, 2048], P('sp', 'tp')
The draws below stay inside these ranges and needn't reach their ends.
All inputs are finite; a program needn't handle non-finite values.
Results may differ from the reference program's by a relative error of at most 0.012.
The reference program's roundings to bfloat16 on the way count: a program that leaves them out, or rounds other values in their place, can miss the bound.
Values may be sent and summed in bfloat16 or wider, within the bound.
A program may use at most 64 MiB of HBM per device.

```python
import jax
import jax.numpy as jnp
from jax import lax

D = 2048
HEADS = 16
KV_HEADS = 4
HEAD_DIM = 64
POOL_GROUPS = 4
GROUP_DIM = 256
WINDOW = 128
SEQ = 65536
ATTN_WIDTH = 1024
KV_WIDTH = 256
POOL_WIDTH = 1024
N_TP = 4


def draw_tokens(key, part):
    base = jnp.clip(jax.random.normal(key, (SEQ, D), jnp.float32), -6.0, 6.0)
    return base.astype(jnp.bfloat16)


def levels(stream_key, dims, pieces, smallest, top_value):
    level = 1.0
    for position, shards_of in pieces:
        heights = jax.random.uniform(jax.random.fold_in(jax.random.fold_in(stream_key, 6), position), (shards_of,), jnp.float32, smallest / len(pieces), top_value / len(pieces))
        level = level * jnp.repeat(jnp.exp(heights), dims[position] // shards_of).reshape((-1,) + (1,) * (len(dims) - 1 - position))
    return level


def centred(rng, shape, deviation, bound, shards=(), kind=jnp.bfloat16):
    entries = jax.random.normal(rng, shape, jnp.float32) * deviation
    if len(shards) > 0:
        entries = levels(rng, shape, shards, -0.22, 0.18) * entries
    return jnp.clip(entries, min=-bound, max=bound).astype(kind)


def setup_inputs(seed: int = 0) -> dict:
    splits = jax.random.split(jax.random.key(seed), 12)
    return {
        "tokens": draw_tokens(jax.random.fold_in(splits[11], 71), 0),
        "w_query": centred(splits[1], (D, ATTN_WIDTH), D ** -0.5, 0.125, ((0, 128), (1, 4))),
        "w_key": centred(splits[2], (D, KV_WIDTH), D ** -0.5, 0.125, ((0, 128), (1, 4))),
        "w_value": centred(splits[3], (D, KV_WIDTH), D ** -0.5, 0.125, ((0, 128), (1, 4))),
        "w_pool_in": centred(splits[4], (D, POOL_WIDTH), D ** -0.5, 0.125, ((0, 128), (1, 4))),
        "sink": jnp.clip(3.0 + 4.0 * jax.random.uniform(splits[5], (HEADS,), jnp.float32) ** levels(splits[5], (HEADS,), ((0, 4),), -0.2, 0.2), 3.0, 7.0),
        "w_pool": centred(splits[6], (POOL_GROUPS, GROUP_DIM, GROUP_DIM), GROUP_DIM ** -0.5, 0.375, ((0, 4),)),
        "pool_scale": jnp.clip(1.0 + 0.18 * jax.random.normal(splits[7], (POOL_WIDTH,), jnp.float32), 0.1, 1.9),
        "w_out_attn": centred(splits[8], (ATTN_WIDTH, D), (ATTN_WIDTH // 8) ** -0.5, 0.5, ((0, 4), (1, 128))),
        "w_out_pool": centred(splits[9], (POOL_WIDTH, D), (ATTN_WIDTH + POOL_WIDTH) ** -0.5, 0.125, ((0, 4), (1, 128))),
        "out_gain": jnp.clip(1.0 + 0.18 * jax.random.normal(splits[10], (D,), jnp.float32), 0.1, 1.9),
    }


epsilon = 1e-05
masked_score = -1e+30

def attend_head(query_one, key_one, value_one, sink_one):
    seq_len = query_one.shape[0]
    group = query_one.shape[1]
    block_count = seq_len // WINDOW
    query_blocks = query_one.reshape(block_count, WINDOW, group, HEAD_DIM).astype(jnp.float32)

    def banded(source):
        padded = jnp.pad(source, ((WINDOW, WINDOW), (0, 0))).reshape(block_count + 2, WINDOW, HEAD_DIM)
        return jnp.concatenate([padded[:-2], padded[1:-1], padded[2:]], axis=1).astype(jnp.float32)
    key_band = banded(key_one)
    value_band = banded(value_one)
    scores = jnp.einsum('nqgd,nsd->ngqs', query_blocks, key_band) * HEAD_DIM ** (-0.5)
    starts = jnp.arange(block_count, dtype=jnp.int32) * WINDOW
    query_pos = starts[:, None] + jnp.arange(WINDOW, dtype=jnp.int32)[None, :]
    key_pos = starts[:, None] + jnp.arange(3 * WINDOW, dtype=jnp.int32)[None, :] - WINDOW
    distance = key_pos[:, None, :] - query_pos[:, :, None]
    inside = (key_pos >= 0) & (key_pos < seq_len)
    keep = (jnp.abs(distance) <= WINDOW) & inside[:, None, :]
    scores = jnp.where(keep[:, None], scores, masked_score)
    sink_logit = sink_one.astype(jnp.float32)[None, :, None, None]
    top = jnp.maximum(lax.optimization_barrier(jnp.max(scores, axis=-1, keepdims=True)), sink_logit)
    raised = jnp.exp(scores - top)
    total = lax.optimization_barrier(jnp.sum(raised, axis=-1, keepdims=True)) + jnp.exp(sink_logit - top)
    probs = (raised / total).astype(jnp.bfloat16)
    attended = jnp.einsum('ngqs,nsd->nqgd', probs.astype(jnp.float32), value_band)
    return attended.astype(jnp.bfloat16).reshape(seq_len, group * HEAD_DIM)

def reference(tokens, w_query, w_key, w_value, w_pool_in, sink, w_pool, pool_scale, w_out_attn, w_out_pool, out_gain):
    seq_len = tokens.shape[0]
    group = HEADS // KV_HEADS
    query = jnp.dot(tokens, w_query, preferred_element_type=jnp.float32).astype(jnp.bfloat16)
    keys = jnp.dot(tokens, w_key, preferred_element_type=jnp.float32).astype(jnp.bfloat16)
    values = jnp.dot(tokens, w_value, preferred_element_type=jnp.float32).astype(jnp.bfloat16)
    chan = jnp.dot(tokens, w_pool_in, preferred_element_type=jnp.float32).astype(jnp.bfloat16)
    query_heads = query.reshape(seq_len, KV_HEADS, group, HEAD_DIM).transpose(1, 0, 2, 3)
    key_heads = keys.reshape(seq_len, KV_HEADS, HEAD_DIM).transpose(1, 0, 2)
    value_heads = values.reshape(seq_len, KV_HEADS, HEAD_DIM).transpose(1, 0, 2)
    sink_heads = sink.reshape(KV_HEADS, group)
    attended = lax.map(lambda parts: attend_head(*parts), (query_heads, key_heads, value_heads, sink_heads))
    attended = attended.transpose(1, 0, 2).reshape(seq_len, HEADS * HEAD_DIM)
    chan_float = chan.astype(jnp.float32)
    running = jnp.concatenate([jnp.zeros((1, POOL_WIDTH), jnp.float32), jnp.cumsum(chan_float, axis=0)], axis=0)
    positions = jnp.arange(seq_len, dtype=jnp.int32)
    outputs = []
    for level in range(POOL_GROUPS):
        half = 2 ** level
        lower = jnp.clip(positions - half, 0, seq_len)
        upper = jnp.clip(positions + half, 0, seq_len)
        columns = slice(level * GROUP_DIM, (level + 1) * GROUP_DIM)
        band = running[:, columns]
        count = (upper - lower).astype(jnp.float32)
        spread = ((band[upper] - band[lower]) / count[:, None] - chan_float[:, columns]).astype(jnp.bfloat16)
        outputs.append(jnp.dot(spread, w_pool[level], preferred_element_type=jnp.float32))
    pooled = (jnp.concatenate(outputs, axis=1) * pool_scale).astype(jnp.bfloat16)
    attn_share = ATTN_WIDTH // N_TP
    pool_share = POOL_WIDTH // N_TP
    mix = jnp.zeros((seq_len, D), jnp.float32)
    for device in range(N_TP):
        attn_cols = slice(device * attn_share, (device + 1) * attn_share)
        pool_cols = slice(device * pool_share, (device + 1) * pool_share)
        partial_sum = jnp.dot(attended[:, attn_cols], w_out_attn[attn_cols], preferred_element_type=jnp.float32)
        partial_sum = partial_sum + jnp.dot(pooled[:, pool_cols], w_out_pool[pool_cols], preferred_element_type=jnp.float32)
        mix = mix + partial_sum.astype(jnp.bfloat16).astype(jnp.float32)
    row_mean = lax.optimization_barrier(jnp.sum(mix, axis=1)) / D
    variance = lax.optimization_barrier(jnp.sum(mix * mix, axis=1)) / D - row_mean * row_mean
    normed = (mix - row_mean[:, None]) * lax.rsqrt(variance + epsilon)[:, None] * out_gain
    return normed.astype(jnp.bfloat16)
```

```python
import jax
import jax.numpy as jnp
from jax import lax
from jax.experimental import pallas as pl
from jax.experimental.pallas import tpu as pltpu
from jax.sharding import Mesh
from jax.sharding import PartitionSpec as P

HEAD_DIM = 64
WINDOW = 128
RIM = 16
SP = ("sp_0", "sp_1", "sp_2")
MESH = pl.DeviceIdType.MESH
NZ, NX, NC, NY = 16, 4, 2, 4

epsilon = 1e-05
masked_score = -1e30

BATCHES = ((0, 5), (12, 16), (5, 8), (8, 12))
NT = (((1,), (1,)), ((), ()))
BF16, F32 = jnp.bfloat16, jnp.float32


def kernel(
    tok_hbm, wq_ref, wk_ref, wv_ref, wc_ref, sink_ref, wpool_ref, scale_ref, woa_ref, wop_ref, gain_ref,
    out_hbm,
    toks, win, wout, win_abs, wout_abs, query, kv, chan, hid, part, comb, relayed, from_prev, from_next,
    share, stats, outv, local_sem, out_sem, send_sem, recv_sem,
):
    z, x, c, y = (lax.axis_index(a) for a in (*SP, "tp"))
    rows, feats = toks.shape[1], toks.shape[2]
    seq_len = rows * NZ * NX * NC
    blocks = rows // WINDOW
    place = (z * NX + x) * NC + c
    offset = place * rows
    total_places = NZ * NX * NC

    def dev_z(d):
        return {"sp_0": lax.rem(z + (d + NZ), NZ)}

    def dev_x(d):
        return {"sp_1": lax.rem(x + (d + NX), NX)}

    def dev_y(d):
        return {"tp": lax.rem(y + (d + NY), NY)}

    dev_c = {"sp_2": 1 - c}

    def dev_sp(d):
        s = lax.rem(place + (d + total_places), total_places)
        return {
            "sp_0": lax.div(s, NX * NC),
            "sp_1": lax.rem(lax.div(s, NC), NX),
            "sp_2": lax.rem(s, NC),
        }

    peers = [dev_z(d) for d in (1, -1, 2, -2, 3, -3, 4, -4)]
    peers += [dev_x(1), dev_x(-1), dev_c, dev_y(1), dev_y(-1), dev_y(2), dev_sp(1), dev_sp(-1)]

    own_tokens = pltpu.make_async_copy(tok_hbm, toks.at[0], local_sem)
    own_tokens.start()
    barrier = pltpu.get_barrier_semaphore()
    for peer in peers:
        pl.semaphore_signal(barrier, inc=1, device_id=peer, device_id_type=MESH)

    win[0, 0, 0, :, 0:256] = wq_ref[...]
    win[0, 0, 0, :, 256:384] = jnp.concatenate([wk_ref[...], wv_ref[...]], axis=1)
    win[0, 0, 0, :, 384:640] = wc_ref[...]
    eye = jnp.where(
        lax.broadcasted_iota(jnp.int32, (16, 16), 0) == lax.broadcasted_iota(jnp.int32, (16, 16), 1), 1.0, 0.0
    ).astype(BF16)
    wout[0, 0, 0, :, 0:256] = lax.dot_general(eye, woa_ref[...], NT, preferred_element_type=F32).astype(BF16)
    wout[0, 0, 0, :, 256:512] = lax.dot_general(eye, wop_ref[...], NT, preferred_element_type=F32).astype(BF16)

    own_tokens.wait()
    pl.semaphore_wait(barrier, len(peers))

    used = []

    def message(src, dst, device):
        m = len(used)
        copy = pltpu.make_async_remote_copy(
            src_ref=src, dst_ref=dst, send_sem=send_sem.at[m], recv_sem=recv_sem.at[m],
            device_id=device, device_id_type=MESH,
        )
        used.append(copy)
        return copy

    class Gather:
        def __init__(self, w):
            self.w = w
            self.slot = {}
            for d in (4, -4, 3, -3, 2, -2, 1, -1):
                self.slot[(-d) % NZ] = message(w.at[0, 0, 0], w.at[0, 0, (-d) % NZ], dev_z(d))
            for e in (4, 3, 2, 1):
                self.slot[12 - e] = message(w.at[0, 0, 12], w.at[0, 0, 12 - e], dev_z(e))
            for e in (3, 2, 1):
                self.slot[4 + e] = message(w.at[0, 0, 4], w.at[0, 0, 4 + e], dev_z(-e))
            self.xp, self.xm, self.xr, self.cc = [], [], [], {}
            for b, (lo, hi) in enumerate(BATCHES):
                at = pl.ds(lo, hi - lo)
                self.xp.append(message(w.at[0, 0, at], w.at[3, 0, at], dev_x(1)))
                self.xm.append(message(w.at[0, 0, at], w.at[1, 0, at], dev_x(-1)))
                if b % 2 == 0:
                    self.xr.append(message(w.at[3, 0, at], w.at[2, 0, at], dev_x(1)))
                else:
                    self.xr.append(message(w.at[1, 0, at], w.at[2, 0, at], dev_x(-1)))
                for r in range(NX):
                    self.cc[r, b] = message(w.at[r, 0, at], w.at[r, 1, at], dev_c)

        def near(self):
            for d in (4, -4, 3, -3, 2, -2, 1, -1):
                self.slot[(-d) % NZ].start()

        def far(self):
            self.slot[12].wait_recv()
            for e in (4, 3, 2, 1):
                self.slot[12 - e].start()
            self.slot[4].wait_recv()
            for e in (3, 2, 1):
                self.slot[4 + e].start()

        def along_x(self, b):
            lo, hi = BATCHES[b]
            for s in range(lo, hi):
                if s not in (0, 4, 12):
                    self.slot[s].wait_recv()
            self.xp[b].start()
            self.xm[b].start()
            self.cc[0, b].start()

        def relay_x(self, b):
            self.xp[b].wait_recv()
            if b % 2 == 0:
                self.xr[b].start()
            self.cc[3, b].start()
            self.xm[b].wait_recv()
            if b % 2 == 1:
                self.xr[b].start()
            self.cc[1, b].start()

        def last_x(self, b):
            self.xr[b].wait_recv()
            self.cc[2, b].start()

        def done(self):
            for b in range(len(BATCHES)):
                for r in (0, 3, 1, 2):
                    self.cc[r, b].wait_recv()

        def in_order(self, dest):
            w = self.w

            def one(j, carry):
                base = lax.rem(z + j, NZ) * (NX * NC * 16)
                for r in range(NX):
                    for k in range(NC):
                        at = base + lax.rem(x + r, NX) * (NC * 16) + lax.rem(c + k, NC) * 16
                        dest[pl.ds(pl.multiple_of(at, 16), 16), :] = w[r, k, j]
                return carry

            lax.fori_loop(0, NZ, one, 0)

    into = Gather(win)
    outof = Gather(wout)

    def chunk(b):
        return pl.ds(b * WINDOW, WINDOW)

    tok_plus = [message(toks.at[0, chunk(b)], toks.at[3, chunk(b)], dev_y(1)) for b in range(4)]
    tok_minus = [message(toks.at[0, chunk(b)], toks.at[1, chunk(b)], dev_y(-1)) for b in range(4)]
    tok_relay = [
        message(toks.at[3, chunk(b)], toks.at[2, chunk(b)], dev_y(1)) if b < 2
        else message(toks.at[1, chunk(b)], toks.at[2, chunk(b)], dev_y(-1))
        for b in range(4)
    ]

    into.near()
    for b in (0, 1):
        tok_plus[b].start()
        tok_minus[b + 2].start()
    for b in (0, 1):
        tok_plus[b + 2].start()
        tok_minus[b].start()
    into.far()
    outof.near()
    tok_plus[0].wait_recv()
    tok_relay[0].start()
    tok_minus[2].wait_recv()
    tok_relay[2].start()
    into.along_x(0)
    into.along_x(1)
    outof.far()
    tok_plus[1].wait_recv()
    tok_relay[1].start()
    tok_minus[3].wait_recv()
    tok_relay[3].start()
    into.along_x(2)
    into.along_x(3)
    for b in range(4):
        into.relay_x(b)
    for b in range(4):
        into.last_x(b)
    outof.along_x(0)
    outof.along_x(1)
    into.done()
    into.in_order(win_abs)
    outof.along_x(2)
    outof.along_x(3)
    for b in (2, 3):
        tok_plus[b].wait_recv()
        tok_minus[b - 2].wait_recv()
    for b in range(4):
        tok_relay[b].wait_recv()

    for m in range(2):
        at = pl.ds(m * 256, 256)
        for lo, hi in ((256, 384), (384, 640), (0, 256)):
            acc = jnp.zeros((256, hi - lo), F32)
            for r in range(NY):
                depth = pl.ds(pl.multiple_of(lax.rem(y + r, NY) * feats, feats), feats)
                acc = acc + jnp.dot(toks[r, at, :], win_abs[depth, lo:hi], preferred_element_type=F32)
            if lo == 256:
                kv[pl.ds(WINDOW + m * 256, 256), :] = acc.astype(BF16)
            elif lo == 384:
                chan[pl.ds(RIM + m * 256, 256), :] = acc.astype(BF16)
            else:
                query[at, :] = (acc * HEAD_DIM ** (-0.5)).astype(BF16)

    kv_next = message(kv.at[pl.ds(rows, WINDOW)], kv.at[pl.ds(0, WINDOW)], dev_sp(1))
    kv_prev = message(kv.at[pl.ds(WINDOW, WINDOW)], kv.at[pl.ds(WINDOW + rows, WINDOW)], dev_sp(-1))
    ch_next = message(chan.at[pl.ds(rows, RIM)], chan.at[pl.ds(0, RIM)], dev_sp(1))
    ch_prev = message(chan.at[pl.ds(RIM, RIM)], chan.at[pl.ds(RIM + rows, RIM)], dev_sp(-1))
    for copy in (kv_next, kv_prev, ch_next, ch_prev):
        copy.start()

    for b in range(4):
        outof.relay_x(b)
    for b in range(4):
        outof.last_x(b)

    half = lax.shift_left(jnp.int32(1), y.astype(jnp.int32))

    def mixers(n):
        at = pl.ds(n * WINDOW, WINDOW)
        first = offset + n * WINDOW
        i = lax.broadcasted_iota(jnp.int32, (WINDOW, 3 * WINDOW), 0)
        j = lax.broadcasted_iota(jnp.int32, (WINDOW, 3 * WINDOW), 1)
        pos = first + j - WINDOW
        keep = (j >= i) & (j <= i + 2 * WINDOW) & (pos >= 0) & (pos < seq_len)
        band = kv[pl.ds(n * WINDOW, 3 * WINDOW), :]
        keys, values = band[:, :HEAD_DIM], band[:, HEAD_DIM:]
        heads = []
        for h in range(4):
            q = query[at, h * HEAD_DIM : (h + 1) * HEAD_DIM]
            scores = lax.dot_general(q, keys, NT, preferred_element_type=F32)
            scores = jnp.where(keep, scores, masked_score)
            sink = sink_ref[h]
            top = jnp.maximum(jnp.max(scores, axis=1, keepdims=True), sink)
            raised = jnp.exp(scores - top)
            total = jnp.sum(raised, axis=1, keepdims=True) + jnp.exp(sink - top)
            probs = (raised * (1.0 / total)).astype(BF16)
            heads.append(jnp.dot(probs, values, preferred_element_type=F32).astype(BF16))
        hid[at, 0:256] = jnp.concatenate(heads, axis=1)

        i = lax.broadcasted_iota(jnp.int32, (WINDOW, WINDOW + 2 * RIM), 0)
        j = lax.broadcasted_iota(jnp.int32, (WINDOW, WINDOW + 2 * RIM), 1) - RIM
        pos = first + j
        member = (j >= i - half) & (j < i + half) & (pos >= 0) & (pos < seq_len)
        member = jnp.where(member, 1.0, 0.0).astype(BF16)
        sums = jnp.dot(member, chan[pl.ds(n * WINDOW, WINDOW + 2 * RIM), :], preferred_element_type=F32)
        t = first + lax.broadcasted_iota(jnp.int32, (WINDOW, 1), 0)
        count = (jnp.minimum(t + half, seq_len) - jnp.maximum(t - half, 0)).astype(F32)
        spread = (sums / count - chan[pl.ds(n * WINDOW + RIM, WINDOW), :].astype(F32)).astype(BF16)
        pooled = jnp.dot(spread, wpool_ref[0], preferred_element_type=F32) * scale_ref[...]
        hid[at, 256:512] = pooled.astype(BF16)

    def partials(n):
        at = pl.ds(n * WINDOW, WINDOW)
        for d in (2, 1, 3, 0):
            cols = pl.ds(pl.multiple_of(lax.rem(y + d, NY) * feats, feats), feats)
            terms = lax.dot_general(hid[at, :], wout_abs[cols, :], NT, preferred_element_type=F32)
            part[d, at, :] = terms.astype(BF16)

    via, straight, joined = {}, {}, {}
    for n in range(4):
        at = chunk(n)
        if n < 2:
            via[n] = message(part.at[2, at], relayed.at[at], dev_y(1))
            straight[n] = message(part.at[3, at], from_next.at[at], dev_y(-1))
            joined[n] = message(comb.at[at], from_prev.at[at], dev_y(1))
        else:
            via[n] = message(part.at[2, at], relayed.at[at], dev_y(-1))
            straight[n] = message(part.at[1, at], from_prev.at[at], dev_y(1))
            joined[n] = message(comb.at[at], from_next.at[at], dev_y(-1))

    def send(n):
        via[n].start()
        straight[n].start()

    def relay(n):
        at = chunk(n)
        via[n].wait_recv()
        mine = part[1 if n < 2 else 3, at, :]
        comb[at, :] = (mine.astype(F32) + relayed[at, :].astype(F32)).astype(BF16)
        joined[n].start()

    mixers(1)
    mixers(2)
    outof.done()
    outof.in_order(wout_abs)
    partials(1)
    send(1)
    partials(2)
    send(2)
    kv_next.wait_recv()
    ch_next.wait_recv()
    mixers(0)
    partials(0)
    send(0)
    kv_prev.wait_recv()
    ch_prev.wait_recv()
    mixers(3)
    relay(1)
    relay(2)
    partials(3)
    send(3)
    relay(0)
    relay(3)

    lane = lax.broadcasted_iota(jnp.int32, (WINDOW, 128), 1)
    for n in (1, 2, 0, 3):
        at = chunk(n)
        straight[n].wait_recv()
        joined[n].wait_recv()
        mix = part[0, at, :].astype(F32) + from_prev[at, :].astype(F32) + from_next[at, :].astype(F32)
        share[at, :] = mix
        one = jnp.sum(mix, axis=1, keepdims=True)
        two = jnp.sum(mix * mix, axis=1, keepdims=True)
        both = jnp.where(lane == 0, one, jnp.where(lane == 1, two, 0.0))
        stats[0, n * 8 : n * 8 + 8, :] = both.T[0:8]

    told = [
        message(stats.at[0], stats.at[3], dev_y(1)),
        message(stats.at[0], stats.at[1], dev_y(-1)),
        message(stats.at[0], stats.at[2], dev_y(2)),
    ]
    for copy in told:
        copy.start()
    for copy in told:
        copy.wait_recv()
    width = feats * NY
    writes = []
    for n in range(4):
        at = chunk(n)
        eight = slice(n * 8, n * 8 + 8)
        both = stats[0, eight, :] + stats[1, eight, :] + stats[2, eight, :] + stats[3, eight, :]
        both = jnp.concatenate([both] * 16, axis=0).T
        mean = both[:, 0:1] / width
        variance = both[:, 1:2] / width - mean * mean
        normed = (share[at, :] - mean) * lax.rsqrt(variance + epsilon) * gain_ref[...]
        outv[at, :] = normed.astype(BF16)
        write = pltpu.make_async_copy(outv.at[at], out_hbm.at[at], out_sem.at[n])
        write.start()
        writes.append(write)
    for copy in used:
        copy.wait_send()
    for write in writes:
        write.wait()


MESSAGES = 2 * (15 + 12 + 16) + 12 + 4 + 12 + 3


def local(tokens, w_query, w_key, w_value, w_pool_in, sink, w_pool, pool_scale, w_out_attn, w_out_pool, out_gain):
    rows, feats = tokens.shape
    vmem = pl.BlockSpec(memory_space=pltpu.VMEM)
    smem = pl.BlockSpec(memory_space=pltpu.SMEM)
    hbm = pl.BlockSpec(memory_space=pl.ANY)
    lanes_in = 640
    lanes_out = 512
    model = feats * NY
    return pl.pallas_call(
        kernel,
        out_shape=jax.ShapeDtypeStruct((rows, feats), BF16),
        in_specs=[hbm, vmem, vmem, vmem, vmem, smem, vmem, vmem, vmem, vmem, vmem],
        out_specs=hbm,
        scratch_shapes=[
            pltpu.VMEM((NY, rows, feats), BF16),
            pltpu.VMEM((NX, NC, NZ, 16, lanes_in), BF16),
            pltpu.VMEM((NX, NC, NZ, 16, lanes_out), BF16),
            pltpu.VMEM((model, lanes_in), BF16),
            pltpu.VMEM((model, lanes_out), BF16),
            pltpu.VMEM((rows, 256), BF16),
            pltpu.VMEM((rows + 2 * WINDOW, 128), BF16),
            pltpu.VMEM((rows + 2 * RIM, 256), BF16),
            pltpu.VMEM((rows, lanes_out), BF16),
            pltpu.VMEM((NY, rows, feats), BF16),
            pltpu.VMEM((rows, feats), BF16),
            pltpu.VMEM((rows, feats), BF16),
            pltpu.VMEM((rows, feats), BF16),
            pltpu.VMEM((rows, feats), BF16),
            pltpu.VMEM((rows, feats), F32),
            pltpu.VMEM((NY, 32, 128), F32),
            pltpu.VMEM((rows, feats), BF16),
            pltpu.SemaphoreType.DMA,
            pltpu.SemaphoreType.DMA((4,)),
            pltpu.SemaphoreType.DMA((MESSAGES,)),
            pltpu.SemaphoreType.DMA((MESSAGES,)),
        ],
        compiler_params=pltpu.CompilerParams(collective_id=0, has_side_effects=True),
    )(
        tokens, w_query, w_key, w_value, w_pool_in, sink, w_pool, pool_scale.reshape(1, -1),
        w_out_attn, w_out_pool, out_gain.reshape(1, -1),
    )


def solution(mesh):
    finer = Mesh(mesh.devices.reshape(NZ, NX, NC, NY), (*SP, "tp"))
    return jax.shard_map(
        local,
        mesh=finer,
        in_specs=(
            P(SP, "tp"), P(SP, "tp"), P(SP, "tp"), P(SP, "tp"), P(SP, "tp"), P("tp"),
            P("tp", None, None), P("tp"), P("tp", SP), P("tp", SP), P("tp"),
        ),
        out_specs=P(SP, "tp"),
        check_vma=False,
    )
```

```python
import jax
import jax.numpy as jnp
from jax import lax
from jax.experimental import pallas as pl
from jax.experimental.pallas import tpu as pltpu
from jax.sharding import Mesh
from jax.sharding import PartitionSpec as P

HEAD_DIM = 64
WINDOW = 128
RIM = 16
SP = ("sp_0", "sp_1", "sp_2")
MESH = pl.DeviceIdType.MESH
NZ, NX, NC, NY = 16, 4, 2, 4

epsilon = 1e-05
masked_score = -1e30

BATCHES = ((0, 1), (1, 5), (12, 16), (5, 8), (8, 12))
OWN, NEAR_A, NEAR_B, FAR_A, FAR_B = range(5)
NT = (((1,), (1,)), ((), ()))
TN = (((0,), (0,)), ((), ()))
BF16, F32 = jnp.bfloat16, jnp.float32


def kernel(
    tok_hbm, wq_hbm, wk_hbm, wv_hbm, wc_hbm, sink_hbm, wpool_hbm, scale_hbm, woa_hbm, wop_hbm, gain_hbm,
    out_hbm,
    toks, win, wout, win_abs, wout_abs, query, kv, chan, hid, part, comb, relayed, from_prev, from_next,
    share, stats, wk, wv, sink, wpool, scale, gain, outv, local_sem, out_sem, send_sem, recv_sem,
):
    z, x, c, y = (lax.axis_index(a) for a in (*SP, "tp"))
    rows, feats = toks.shape[1], toks.shape[2]
    seq_len = rows * NZ * NX * NC
    place = (z * NX + x) * NC + c
    offset = place * rows
    total_places = NZ * NX * NC

    def dev_z(d):
        return {"sp_0": lax.rem(z + (d + NZ), NZ)}

    def dev_x(d):
        return {"sp_1": lax.rem(x + (d + NX), NX)}

    def dev_y(d):
        return {"tp": lax.rem(y + (d + NY), NY)}

    dev_c = {"sp_2": 1 - c}

    def dev_sp(d):
        s = lax.rem(place + (d + total_places), total_places)
        return {
            "sp_0": lax.div(s, NX * NC),
            "sp_1": lax.rem(lax.div(s, NC), NX),
            "sp_2": lax.rem(s, NC),
        }

    peers = [dev_z(d) for d in (4, -4, 3, -3, 2, -2, 1, -1)]
    peers += [dev_y(2), dev_x(2), dev_sp(1), dev_sp(-1), dev_x(1), dev_x(-1), dev_y(1), dev_y(-1), dev_c]
    barrier = pltpu.get_barrier_semaphore()
    for peer in peers:
        pl.semaphore_signal(barrier, inc=1, device_id=peer, device_id_type=MESH)

    mine_in, mine_out = win.at[0, 0, 0], wout.at[0, 0, 0]
    pairs = (
        (wk_hbm, wk), (wv_hbm, wv), (wq_hbm, mine_in.at[:, pl.ds(0, 256)]), (wc_hbm, mine_in.at[:, pl.ds(384, 256)]),
        (tok_hbm, toks.at[0]), (woa_hbm, mine_out.at[:, pl.ds(0, 256)]), (wop_hbm, mine_out.at[:, pl.ds(256, 256)]),
        (wpool_hbm, wpool), (scale_hbm, scale), (gain_hbm, gain), (sink_hbm, sink),
    )
    loads = [pltpu.make_async_copy(a, b, local_sem.at[k]) for k, (a, b) in enumerate(pairs)]
    for load in loads:
        load.start()

    with jax.named_scope("entry"):
        loads[0].wait()
        loads[1].wait()
        win[0, 0, 0, :, 256:384] = jnp.concatenate([wk[...], wv[...]], axis=1)
        for load in loads[2:]:
            load.wait()
        pl.semaphore_wait(barrier, len(peers))

    used = []

    def message(src, dst, device):
        m = len(used)
        copy = pltpu.make_async_remote_copy(
            src_ref=src, dst_ref=dst, send_sem=send_sem.at[m], recv_sem=recv_sem.at[m],
            device_id=device, device_id_type=MESH,
        )
        used.append(copy)
        return copy

    class Gather:
        def __init__(self, w):
            self.w = w
            self.slot = {}
            for d in (4, -4, 3, -3, 2, -2, 1, -1):
                self.slot[(-d) % NZ] = message(w.at[0, 0, 0], w.at[0, 0, (-d) % NZ], dev_z(d))
            for e in (4, 3, 2, 1):
                self.slot[12 - e] = message(w.at[0, 0, 12], w.at[0, 0, 12 - e], dev_z(e))
            for e in (3, 2, 1):
                self.slot[4 + e] = message(w.at[0, 0, 4], w.at[0, 0, 4 + e], dev_z(-e))
            self.xp, self.xm, self.xr, self.cc = [], [], [], {}
            for b, (lo, hi) in enumerate(BATCHES):
                at = pl.ds(lo, hi - lo)
                self.xp.append(message(w.at[0, 0, at], w.at[3, 0, at], dev_x(1)))
                self.xm.append(message(w.at[0, 0, at], w.at[1, 0, at], dev_x(-1)))
                if b == OWN:
                    self.xr.append(message(w.at[0, 0, at], w.at[2, 0, at], dev_x(2)))
                elif b in (NEAR_A, FAR_A):
                    self.xr.append(message(w.at[3, 0, at], w.at[2, 0, at], dev_x(1)))
                else:
                    self.xr.append(message(w.at[1, 0, at], w.at[2, 0, at], dev_x(-1)))
                for r in range(NX):
                    self.cc[r, b] = message(w.at[r, 0, at], w.at[r, 1, at], dev_c)

        def near(self):
            for d in (4, -4, 3, -3, 2, -2, 1, -1):
                self.slot[(-d) % NZ].start()

        def own(self):
            self.xp[OWN].start()
            self.xm[OWN].start()
            self.xr[OWN].start()
            self.cc[0, OWN].start()

        def far(self):
            self.slot[12].wait_recv()
            for e in (4, 3, 2, 1):
                self.slot[12 - e].start()
            self.slot[4].wait_recv()
            for e in (3, 2, 1):
                self.slot[4 + e].start()

        def along_x(self, b):
            lo, hi = BATCHES[b]
            for s in range(lo, hi):
                if s not in (4, 12):
                    self.slot[s].wait_recv()
            self.xp[b].start()
            self.xm[b].start()
            self.cc[0, b].start()

        def relay_x(self, b):
            self.xp[b].wait_recv()
            if b in (NEAR_A, FAR_A):
                self.xr[b].start()
            self.cc[3, b].start()
            self.xm[b].wait_recv()
            if b in (NEAR_B, FAR_B):
                self.xr[b].start()
            self.cc[1, b].start()

        def last_x(self, b):
            self.xr[b].wait_recv()
            self.cc[2, b].start()

        def in_order(self, dest, b):
            w = self.w
            for r in (0, 3, 1, 2):
                self.cc[r, b].wait_recv()

            def one(j, carry):
                base = lax.rem(z + j, NZ) * (NX * NC * 16)
                for r in range(NX):
                    for k in range(NC):
                        at = base + lax.rem(x + r, NX) * (NC * 16) + lax.rem(c + k, NC) * 16
                        dest[pl.ds(pl.multiple_of(at, 16), 16), :] = w[r, k, j]
                return carry

            lax.fori_loop(*BATCHES[b], one, 0)

    into = Gather(win)
    outof = Gather(wout)

    def chunk(b):
        return pl.ds(b * WINDOW, WINDOW)

    tok_plus = [message(toks.at[0, chunk(b)], toks.at[3, chunk(b)], dev_y(1)) for b in range(4)]
    tok_minus = [message(toks.at[0, chunk(b)], toks.at[1, chunk(b)], dev_y(-1)) for b in range(4)]
    tok_relay = [
        message(toks.at[3, chunk(b)], toks.at[2, chunk(b)], dev_y(1)) if b < 2
        else message(toks.at[1, chunk(b)], toks.at[2, chunk(b)], dev_y(-1))
        for b in range(4)
    ]

    with jax.named_scope("near"):
        into.near()
        into.own()
        for b in (0, 1):
            tok_plus[b].start()
            tok_minus[b + 2].start()
        for b in (0, 1):
            tok_plus[b + 2].start()
            tok_minus[b].start()
    with jax.named_scope("in_far"):
        into.far()
        outof.near()
    with jax.named_scope("in_x_near"):
        into.along_x(NEAR_A)
        into.along_x(NEAR_B)
        outof.own()
    with jax.named_scope("tok_relay_a"):
        tok_plus[0].wait_recv()
        tok_relay[0].start()
        tok_minus[2].wait_recv()
        tok_relay[2].start()
        into.relay_x(OWN)
        into.last_x(OWN)
    with jax.named_scope("in_x_relay_near"):
        into.relay_x(NEAR_A)
        into.relay_x(NEAR_B)
    with jax.named_scope("tok_relay_b"):
        tok_plus[1].wait_recv()
        tok_relay[1].start()
        tok_minus[3].wait_recv()
        tok_relay[3].start()
    with jax.named_scope("in_x_far"):
        into.along_x(FAR_A)
        into.along_x(FAR_B)
        outof.relay_x(OWN)
        outof.last_x(OWN)
    with jax.named_scope("out_far"):
        outof.far()
    with jax.named_scope("in_x_relay_far"):
        into.relay_x(FAR_A)
        into.relay_x(FAR_B)
    with jax.named_scope("out_x_near"):
        outof.along_x(NEAR_A)
        outof.along_x(NEAR_B)
    with jax.named_scope("in_last"):
        for b in (NEAR_A, NEAR_B):
            into.last_x(b)
        for b in (OWN, NEAR_A, NEAR_B):
            into.in_order(win_abs, b)
        for b in (FAR_A, FAR_B):
            into.last_x(b)
    with jax.named_scope("out_x_relay_near"):
        outof.relay_x(NEAR_A)
        outof.relay_x(NEAR_B)
    with jax.named_scope("in_order"):
        for b in (FAR_A, FAR_B):
            into.in_order(win_abs, b)
    with jax.named_scope("tok_done"):
        for b in (2, 3):
            tok_plus[b].wait_recv()
            tok_minus[b - 2].wait_recv()
        for b in range(4):
            tok_relay[b].wait_recv()

    with jax.named_scope("project"):
        for lo, hi in ((256, 384), (384, 640), (0, 256)):
            acc = jnp.zeros((rows, hi - lo), F32)
            for r in range(NY):
                depth = pl.ds(pl.multiple_of(lax.rem(y + r, NY) * feats, feats), feats)
                acc = acc + jnp.dot(toks[r], win_abs[depth, lo:hi], preferred_element_type=F32)
            if lo == 256:
                kv[pl.ds(WINDOW, rows), :] = acc.astype(BF16)
            elif lo == 384:
                chan[pl.ds(RIM, rows), :] = acc.astype(BF16)
            else:
                query[...] = (acc * HEAD_DIM ** (-0.5)).astype(BF16)

    kv_next = message(kv.at[pl.ds(rows, WINDOW)], kv.at[pl.ds(0, WINDOW)], dev_sp(1))
    kv_prev = message(kv.at[pl.ds(WINDOW, WINDOW)], kv.at[pl.ds(WINDOW + rows, WINDOW)], dev_sp(-1))
    ch_next = message(chan.at[pl.ds(rows, RIM)], chan.at[pl.ds(0, RIM)], dev_sp(1))
    ch_prev = message(chan.at[pl.ds(RIM, RIM)], chan.at[pl.ds(RIM + rows, RIM)], dev_sp(-1))
    halos = (kv_next, kv_prev, ch_next, ch_prev)
    for copy in halos:
        copy.start()

    with jax.named_scope("out_x_far"):
        outof.along_x(FAR_A)
        outof.along_x(FAR_B)

    half = lax.shift_left(jnp.int32(1), y.astype(jnp.int32))
    sinks = jnp.concatenate([jnp.broadcast_to(sink[0:1, h : h + 1], (1, WINDOW)) for h in range(4)], axis=1)

    def attend(n):
        first = offset + n * WINDOW
        band = kv[pl.ds(n * WINDOW, 3 * WINDOW), :]
        keys, values = band[:, :HEAD_DIM], band[:, HEAD_DIM:]
        block = query[n * WINDOW : (n + 1) * WINDOW, :]
        stacked = jnp.concatenate([block[:, h * HEAD_DIM : (h + 1) * HEAD_DIM] for h in range(4)], axis=0)
        scores = lax.dot_general(keys, stacked, NT, preferred_element_type=F32)
        j = lax.broadcasted_iota(jnp.int32, (WINDOW, 4 * WINDOW), 0)
        i = lax.rem(lax.broadcasted_iota(jnp.int32, (WINDOW, 4 * WINDOW), 1), WINDOW)
        before = jnp.where((j >= i) & (first > 0), scores[:WINDOW], masked_score)
        here = scores[WINDOW : 2 * WINDOW]
        after = jnp.where((j <= i) & (first + WINDOW < seq_len), scores[2 * WINDOW :], masked_score)
        top = jnp.max(jnp.maximum(jnp.maximum(before, here), after), axis=0, keepdims=True)
        top = jnp.maximum(top, sinks)
        before, here, after = jnp.exp(before - top), jnp.exp(here - top), jnp.exp(after - top)
        total = jnp.sum(before + here + after, axis=0, keepdims=True) + jnp.exp(sinks - top)
        inverse = 1.0 / total
        probs = jnp.concatenate([(r * inverse).astype(BF16) for r in (before, here, after)], axis=0)
        out = lax.dot_general(values, probs, TN, preferred_element_type=F32)
        out = jnp.concatenate([out[:, h * WINDOW : (h + 1) * WINDOW] for h in range(4)], axis=0)
        hid[n * WINDOW : (n + 1) * WINDOW, 0:256] = out.T.astype(BF16)

    def pool(n):
        first = offset + n * WINDOW
        i = lax.broadcasted_iota(jnp.int32, (WINDOW, WINDOW + 2 * RIM), 0)
        j = lax.broadcasted_iota(jnp.int32, (WINDOW, WINDOW + 2 * RIM), 1) - RIM
        pos = first + j
        member = (j >= i - half) & (j < i + half) & (pos >= 0) & (pos < seq_len)
        member = jnp.where(member, 1.0, 0.0).astype(BF16)
        sums = jnp.dot(member, chan[pl.ds(n * WINDOW, WINDOW + 2 * RIM), :], preferred_element_type=F32)
        t = first + lax.broadcasted_iota(jnp.int32, (WINDOW, 1), 0)
        count = (jnp.minimum(t + half, seq_len) - jnp.maximum(t - half, 0)).astype(F32)
        spread = (sums / count - chan[pl.ds(n * WINDOW + RIM, WINDOW), :].astype(F32)).astype(BF16)
        pooled = jnp.dot(spread, wpool[0], preferred_element_type=F32) * scale[...]
        hid[n * WINDOW : (n + 1) * WINDOW, 256:512] = pooled.astype(BF16)

    def mixers(first, second):
        for n in (first, second):
            pool(n)
            attend(n)

    def partials(first, second):
        both = jnp.concatenate([hid[chunk(first), :], hid[chunk(second), :]], axis=0)
        for d in (2, 1, 3, 0):
            cols = pl.ds(pl.multiple_of(lax.rem(y + d, NY) * feats, feats), feats)
            terms = lax.dot_general(both, wout_abs[cols, :], NT, preferred_element_type=F32).astype(BF16)
            part[d, chunk(first), :] = terms[:WINDOW]
            part[d, chunk(second), :] = terms[WINDOW:]

    via, straight, joined = {}, {}, {}
    for n in range(4):
        at = chunk(n)
        if n < 2:
            via[n] = message(part.at[2, at], relayed.at[at], dev_y(1))
            straight[n] = message(part.at[3, at], from_next.at[at], dev_y(-1))
            joined[n] = message(comb.at[at], from_prev.at[at], dev_y(1))
        else:
            via[n] = message(part.at[2, at], relayed.at[at], dev_y(-1))
            straight[n] = message(part.at[1, at], from_prev.at[at], dev_y(1))
            joined[n] = message(comb.at[at], from_next.at[at], dev_y(-1))

    def send(first, second):
        for copy in (via[first], via[second], straight[first], straight[second]):
            copy.start()

    def relay(n):
        at = chunk(n)
        via[n].wait_recv()
        mine = part[1 if n < 2 else 3, at, :]
        comb[at, :] = (mine.astype(F32) + relayed[at, :].astype(F32)).astype(BF16)
        joined[n].start()

    with jax.named_scope("mix12"):
        mixers(1, 2)
    with jax.named_scope("out_x_relay_far"):
        outof.relay_x(FAR_A)
        outof.relay_x(FAR_B)
    with jax.named_scope("halo"):
        for copy in halos:
            copy.wait_recv()
    with jax.named_scope("mix03"):
        mixers(0, 3)
    with jax.named_scope("out_last"):
        for b in (NEAR_A, NEAR_B):
            outof.last_x(b)
        for b in (OWN, NEAR_A, NEAR_B):
            outof.in_order(wout_abs, b)
        for b in (FAR_A, FAR_B):
            outof.last_x(b)
        for b in (FAR_A, FAR_B):
            outof.in_order(wout_abs, b)
    with jax.named_scope("part12"):
        partials(1, 2)
        send(1, 2)
    with jax.named_scope("part03"):
        partials(0, 3)
        send(0, 3)
    with jax.named_scope("relay12"):
        relay(1)
        relay(2)
    with jax.named_scope("relay03"):
        relay(0)
        relay(3)

    lane = lax.broadcasted_iota(jnp.int32, (WINDOW, 128), 1)
    told = []

    def settle(p, first, second):
        for k, n in enumerate((first, second)):
            at = chunk(n)
            straight[n].wait_recv()
            joined[n].wait_recv()
            mix = part[0, at, :].astype(F32) + from_prev[at, :].astype(F32) + from_next[at, :].astype(F32)
            share[at, :] = mix
            one = jnp.sum(mix, axis=1, keepdims=True)
            two = jnp.sum(mix * mix, axis=1, keepdims=True)
            both = jnp.where(lane == 0, one, jnp.where(lane == 1, two, 0.0))
            stats[0, p, k * 8 : k * 8 + 8, :] = both.T[0:8]
        told.append([
            message(stats.at[0, p], stats.at[2, p], dev_y(2)),
            message(stats.at[0, p], stats.at[3, p], dev_y(1)),
            message(stats.at[0, p], stats.at[1, p], dev_y(-1)),
        ])
        for copy in told[p]:
            copy.start()

    width = feats * NY
    writes = []

    def finish(p, first, second):
        for copy in told[p]:
            copy.wait_recv()
        for k, n in enumerate((first, second)):
            at = chunk(n)
            eight = slice(k * 8, k * 8 + 8)
            both = stats[0, p, eight, :] + stats[1, p, eight, :] + stats[2, p, eight, :] + stats[3, p, eight, :]
            both = jnp.concatenate([both] * 16, axis=0).T
            mean = both[:, 0:1] / width
            variance = both[:, 1:2] / width - mean * mean
            normed = (share[at, :] - mean) * lax.rsqrt(variance + epsilon) * gain[...]
            outv[at, :] = normed.astype(BF16)
            writes.append(pltpu.make_async_copy(outv.at[at], out_hbm.at[at], out_sem.at[n]))
            writes[-1].start()

    with jax.named_scope("settle12"):
        settle(0, 1, 2)
    with jax.named_scope("settle03"):
        settle(1, 0, 3)
    with jax.named_scope("finish12"):
        finish(0, 1, 2)
        for copy in used:
            copy.wait_send()
    with jax.named_scope("finish03"):
        finish(1, 0, 3)
        for write in writes:
            write.wait()


MESSAGES = 2 * (15 + 15 + 20) + 12 + 4 + 12 + 6


def local(tokens, w_query, w_key, w_value, w_pool_in, sink, w_pool, pool_scale, w_out_attn, w_out_pool, out_gain):
    rows, feats = tokens.shape
    hbm = pl.BlockSpec(memory_space=pltpu.HBM)
    lanes_in = 640
    lanes_out = 512
    model = feats * NY
    return pl.pallas_call(
        kernel,
        out_shape=jax.ShapeDtypeStruct((rows, feats), BF16),
        in_specs=[hbm] * 11,
        out_specs=hbm,
        scratch_shapes=[
            pltpu.VMEM((NY, rows, feats), BF16),
            pltpu.VMEM((NX, NC, NZ, 16, lanes_in), BF16),
            pltpu.VMEM((NX, NC, NZ, 16, lanes_out), BF16),
            pltpu.VMEM((model, lanes_in), BF16),
            pltpu.VMEM((model, lanes_out), BF16),
            pltpu.VMEM((rows, 256), BF16),
            pltpu.VMEM((rows + 2 * WINDOW, 128), BF16),
            pltpu.VMEM((rows + 2 * RIM, 256), BF16),
            pltpu.VMEM((rows, lanes_out), BF16),
            pltpu.VMEM((NY, rows, feats), BF16),
            pltpu.VMEM((rows, feats), BF16),
            pltpu.VMEM((rows, feats), BF16),
            pltpu.VMEM((rows, feats), BF16),
            pltpu.VMEM((rows, feats), BF16),
            pltpu.VMEM((rows, feats), F32),
            pltpu.VMEM((NY, 2, 16, 128), F32),
            pltpu.VMEM((16, 64), BF16),
            pltpu.VMEM((16, 64), BF16),
            pltpu.VMEM((1, 4), F32),
            pltpu.VMEM((1, 256, 256), BF16),
            pltpu.VMEM((1, 256), F32),
            pltpu.VMEM((1, 512), F32),
            pltpu.VMEM((rows, feats), BF16),
            pltpu.SemaphoreType.DMA((11,)),
            pltpu.SemaphoreType.DMA((4,)),
            pltpu.SemaphoreType.DMA((MESSAGES,)),
            pltpu.SemaphoreType.DMA((MESSAGES,)),
        ],
        compiler_params=pltpu.CompilerParams(
            collective_id=0, has_side_effects=True
        ),
    )(
        tokens, w_query, w_key, w_value, w_pool_in, sink.reshape(1, -1), w_pool, pool_scale.reshape(1, -1),
        w_out_attn.T, w_out_pool.T, out_gain.reshape(1, -1),
    )


def solution(mesh):
    finer = Mesh(mesh.devices.reshape(NZ, NX, NC, NY), (*SP, "tp"))
    return jax.shard_map(
        local,
        mesh=finer,
        in_specs=(
            P(SP, "tp"), P(SP, "tp"), P(SP, "tp"), P(SP, "tp"), P(SP, "tp"), P("tp"),
            P("tp", None, None), P("tp"), P("tp", SP), P("tp", SP), P("tp"),
        ),
        out_specs=P(SP, "tp"),
        check_vma=False,
    )
```

```python
import jax
import jax.numpy as jnp
from jax import lax
from jax.experimental import pallas as pl
from jax.experimental.pallas import tpu as pltpu
from jax.sharding import Mesh
from jax.sharding import PartitionSpec as P

HEAD_DIM = 64
WINDOW = 128
RIM = 16
SP = ("sp_0", "sp_1", "sp_2")
MESH = pl.DeviceIdType.MESH
NZ, NX, NC, NY = 16, 4, 2, 4

epsilon = 1e-05
masked_score = -1e30

OWN, NEAR, FAR = 4, (0, 9), (9, 16)
FIRST, LOW, HIGH = (2, 7), (0, 2), (7, 9)
NT = (((1,), (1,)), ((), ()))
TN = (((0,), (0,)), ((), ()))
BF16, F32 = jnp.bfloat16, jnp.float32


def kernel(
    tok_hbm, wq_hbm, wk_hbm, wv_hbm, wc_hbm, sink_hbm, wpool_hbm, scale_hbm, woa_hbm, wop_hbm, gain_hbm,
    out_hbm,
    toks, win, wout, win_abs, wout_abs, query, kv, chan, hid, part, comb, relayed, from_prev, from_next,
    share, stats, wk, wv, sink, wpool, scale, gain, outv, local_sem, out_sem, sems,
):
    z, x, c, y = (lax.axis_index(a) for a in (*SP, "tp"))
    rows, feats = toks.shape[1], toks.shape[2]
    seq_len = rows * NZ * NX * NC
    place = (z * NX + x) * NC + c
    offset = place * rows
    total_places = NZ * NX * NC

    def dev_z(d):
        return {"sp_0": lax.rem(z + (d + NZ), NZ)}

    def dev_x(d):
        return {"sp_1": lax.rem(x + (d + NX), NX)}

    def dev_y(d):
        return {"tp": lax.rem(y + (d + NY), NY)}

    dev_c = {"sp_2": 1 - c}

    def dev_sp(d):
        s = lax.rem(place + (d + total_places), total_places)
        return {
            "sp_0": lax.div(s, NX * NC),
            "sp_1": lax.rem(lax.div(s, NC), NX),
            "sp_2": lax.rem(s, NC),
        }

    peers = [dev_z(d) for d in (4, -4, 3, -3, 2, -2, 1, -1)]
    peers += [dev_y(2), dev_x(2), dev_sp(1), dev_sp(-1), dev_x(1), dev_x(-1), dev_y(1), dev_y(-1), dev_c]
    barrier = pltpu.get_barrier_semaphore()
    for peer in peers:
        pl.semaphore_signal(barrier, inc=1, device_id=peer, device_id_type=MESH)

    mine_in, mine_out = win.at[OWN], wout.at[OWN]
    pairs = (
        (wk_hbm, wk), (wv_hbm, wv), (wq_hbm, mine_in.at[:, pl.ds(0, 256)]), (wc_hbm, mine_in.at[:, pl.ds(384, 256)]),
        (tok_hbm, toks.at[0]), (woa_hbm, mine_out.at[:, pl.ds(0, 256)]), (wop_hbm, mine_out.at[:, pl.ds(256, 256)]),
        (wpool_hbm, wpool), (scale_hbm, scale), (gain_hbm, gain), (sink_hbm, sink),
    )
    loads = [pltpu.make_async_copy(a, b, local_sem.at[k]) for k, (a, b) in enumerate(pairs)]
    for load in loads:
        load.start()

    with jax.named_scope("entry"):
        loads[0].wait()
        loads[1].wait()
        win[OWN, :, 256:384] = jnp.concatenate([wk[...], wv[...]], axis=1)
        for load in loads[2:]:
            load.wait()
        pl.semaphore_wait(barrier, len(peers))

    groups = {}

    def message(src, dst, device, sent, got):
        for key in (("send", sent), ("recv", got)):
            groups.setdefault(key, len(groups))
        return pltpu.make_async_remote_copy(
            src_ref=src, dst_ref=dst, send_sem=sems.at[groups["send", sent]], recv_sem=sems.at[groups["recv", got]],
            device_id=device, device_id_type=MESH,
        )

    def waiting(ref, kind, name):
        sem = sems.at[groups[kind, name]]
        copy = pltpu.make_async_remote_copy(
            src_ref=ref, dst_ref=ref, send_sem=sem, recv_sem=sem, device_id=dev_c, device_id_type=MESH
        )
        if kind == "send":
            copy.wait_send()
        else:
            copy.wait_recv()

    class Gather:
        def __init__(self, w, name):
            self.w, self.name = w, name

        def at(self, r, k, lo, hi):
            return self.w.at[pl.ds((r * NC + k) * NZ + lo, hi - lo)]

        def send(self, src, dst, device, got):
            message(src, dst, device, self.name, self.name + got).start()

        def wait(self, slots, got):
            waiting(self.w.at[pl.ds(0, slots)], "recv", self.name + got)

        def near(self):
            for d in (4, -4, 2, -2, 1, -1, 3, -3):
                p = (4 - d) % NZ
                got = {4: "m4", -4: "p4", 3: "n3", -3: "n3"}.get(d, "n1")
                self.send(self.at(0, 0, OWN, OWN + 1), self.at(0, 0, p, p + 1), dev_z(d), got)

        def far(self):
            self.wait(1, "m4")
            for e in (4, 3, 2, 1):
                self.send(self.at(0, 0, 0, 1), self.at(0, 0, 16 - e, 17 - e), dev_z(e), "far")
            self.wait(1, "p4")
            for e in (3, 2, 1):
                self.send(self.at(0, 0, 8, 9), self.at(0, 0, 8 + e, 9 + e), dev_z(-e), "far")

        def along_x(self, span):
            self.send(self.at(0, 0, *span), self.at(3, 0, *span), dev_x(1), "xp%d" % span[0])
            self.send(self.at(0, 0, *span), self.at(1, 0, *span), dev_x(-1), "xm%d" % span[0])

        def wait_x(self, r, span):
            self.wait(span[1] - span[0], ("xp%d" if r == 3 else "xm%d") % span[0])

        def relay_x(self, r, span):
            part = "near" if span[0] < 9 else "rest"
            self.send(self.at(r, 0, *span), self.at(2, 0, *span), dev_x(1 if r == 3 else -1), "x2" + part)

        def across(self, r, span):
            part = "near" if span[0] < 9 else "rest"
            self.send(self.at(r, 0, *span), self.at(r, 1, *span), dev_c, "c" + part)

        def first(self):
            self.wait(4, "n1")
            self.along_x(FIRST)

        def second(self):
            self.wait(2, "n3")
            self.along_x(LOW)
            self.along_x(HIGH)
            self.across(0, NEAR)

        def third(self):
            self.wait(7, "far")
            self.along_x(FAR)
            self.across(0, FAR)

        def relay_first(self):
            self.wait_x(3, FIRST)
            self.relay_x(3, (2, 5))
            self.wait_x(1, FIRST)
            self.relay_x(1, (5, 7))

        def relay_second(self):
            self.wait_x(3, LOW)
            self.relay_x(3, LOW)
            self.wait_x(1, HIGH)
            self.relay_x(1, HIGH)
            self.wait_x(3, HIGH)
            self.across(3, NEAR)
            self.wait_x(1, LOW)
            self.across(1, NEAR)

        def relay_third(self):
            self.wait_x(3, FAR)
            self.relay_x(3, (9, 12))
            self.across(3, FAR)
            self.wait_x(1, FAR)
            self.relay_x(1, (12, 16))
            self.across(1, FAR)

        def last_near(self):
            self.wait(9, "x2near")
            self.across(2, NEAR)

        def last_far(self):
            self.wait(7, "x2rest")
            self.across(2, FAR)

        def in_order(self, dest, span):
            w = self.w
            self.wait(NX * (span[1] - span[0]), "cnear" if span[0] < 9 else "crest")

            def one(p, carry):
                base = lax.rem(z + p + (NZ - 4), NZ) * (NX * NC * 16)
                for r in range(NX):
                    for k in range(NC):
                        at = base + lax.rem(x + r, NX) * (NC * 16) + lax.rem(c + k, NC) * 16
                        dest[pl.ds(pl.multiple_of(at, 16), 16), :] = w[(r * NC + k) * NZ + p]
                return carry

            lax.fori_loop(*span, one, 0)

        def sent(self):
            waiting(self.w.at[pl.ds(0, 127)], "send", self.name)

    into = Gather(win, "in")
    outof = Gather(wout, "out")

    def chunk(b):
        return pl.ds(b * WINDOW, WINDOW)

    def tokens_to(slot, b, src, d, got):
        message(toks.at[src, chunk(b)], toks.at[slot, chunk(b)], dev_y(d), "tok", got).start()

    def tokens_relay(b):
        waiting(toks.at[0, chunk(0)], "recv", "tok%d" % b)
        if b < 2:
            tokens_to(2, b, 3, 1, "tok")
        else:
            tokens_to(2, b, 1, -1, "tok")

    with jax.named_scope("near"):
        into.near()
        for b in (0, 1):
            tokens_to(3, b, 0, 1, "tok%d" % b)
            tokens_to(1, b + 2, 0, -1, "tok%d" % (b + 2))
        for b in (0, 1):
            tokens_to(3, b + 2, 0, 1, "tok")
            tokens_to(1, b, 0, -1, "tok")
    with jax.named_scope("in_first"):
        into.first()
    with jax.named_scope("in_far"):
        into.far()
        outof.near()
    with jax.named_scope("in_second"):
        into.second()
    with jax.named_scope("tok_relay_a"):
        tokens_relay(0)
        tokens_relay(2)
    with jax.named_scope("in_relay_first"):
        into.relay_first()
    with jax.named_scope("tok_relay_b"):
        tokens_relay(1)
        tokens_relay(3)
    with jax.named_scope("in_relay_second"):
        into.relay_second()
    with jax.named_scope("in_third"):
        into.third()
    with jax.named_scope("out_far"):
        outof.far()
    with jax.named_scope("in_last_near"):
        into.last_near()
    with jax.named_scope("in_relay_third"):
        into.relay_third()
    with jax.named_scope("out_first"):
        outof.first()
        outof.second()
    with jax.named_scope("in_order_near"):
        into.in_order(win_abs, NEAR)
    with jax.named_scope("out_third"):
        outof.third()
    with jax.named_scope("in_last_far"):
        into.last_far()
    with jax.named_scope("in_order_far"):
        into.in_order(win_abs, FAR)
    with jax.named_scope("tok_done"):
        waiting(toks.at[pl.ds(0, 2)], "recv", "tok")

    with jax.named_scope("project"):
        for lo, hi in ((256, 384), (384, 640), (0, 256)):
            acc = jnp.zeros((rows, hi - lo), F32)
            for r in range(NY):
                depth = pl.ds(pl.multiple_of(lax.rem(y + r, NY) * feats, feats), feats)
                acc = acc + jnp.dot(toks[r], win_abs[depth, lo:hi], preferred_element_type=F32)
            if lo == 256:
                kv[pl.ds(WINDOW, rows), :] = acc.astype(BF16)
            elif lo == 384:
                chan[pl.ds(RIM, rows), :] = acc.astype(BF16)
            else:
                query[...] = (acc * HEAD_DIM ** (-0.5)).astype(BF16)

    own_kv, own_ch = (kv, WINDOW, "kv"), (chan, RIM, "ch")
    for ref, size, name in (own_kv, own_ch):
        message(ref.at[pl.ds(rows, size)], ref.at[pl.ds(0, size)], dev_sp(1), name, name).start()
        message(ref.at[pl.ds(size, size)], ref.at[pl.ds(size + rows, size)], dev_sp(-1), name, name).start()

    with jax.named_scope("out_relay_first"):
        outof.relay_first()
        outof.relay_second()

    half = lax.shift_left(jnp.int32(1), y.astype(jnp.int32))
    sinks = jnp.concatenate([jnp.broadcast_to(sink[0:1, h : h + 1], (1, WINDOW)) for h in range(4)], axis=1)

    def attend(n):
        first = offset + n * WINDOW
        band = kv[pl.ds(n * WINDOW, 3 * WINDOW), :]
        keys, values = band[:, :HEAD_DIM], band[:, HEAD_DIM:]
        block = query[n * WINDOW : (n + 1) * WINDOW, :]
        stacked = jnp.concatenate([block[:, h * HEAD_DIM : (h + 1) * HEAD_DIM] for h in range(4)], axis=0)
        scores = lax.dot_general(keys, stacked, NT, preferred_element_type=F32)
        j = lax.broadcasted_iota(jnp.int32, (WINDOW, 4 * WINDOW), 0)
        i = lax.rem(lax.broadcasted_iota(jnp.int32, (WINDOW, 4 * WINDOW), 1), WINDOW)
        before = jnp.where((j >= i) & (first > 0), scores[:WINDOW], masked_score)
        here = scores[WINDOW : 2 * WINDOW]
        after = jnp.where((j <= i) & (first + WINDOW < seq_len), scores[2 * WINDOW :], masked_score)
        top = jnp.max(jnp.maximum(jnp.maximum(before, here), after), axis=0, keepdims=True)
        top = jnp.maximum(top, sinks)
        before, here, after = jnp.exp(before - top), jnp.exp(here - top), jnp.exp(after - top)
        total = jnp.sum(before + here + after, axis=0, keepdims=True) + jnp.exp(sinks - top)
        inverse = 1.0 / total
        probs = jnp.concatenate([(r * inverse).astype(BF16) for r in (before, here, after)], axis=0)
        out = lax.dot_general(values, probs, TN, preferred_element_type=F32)
        out = jnp.concatenate([out[:, h * WINDOW : (h + 1) * WINDOW] for h in range(4)], axis=0)
        hid[n * WINDOW : (n + 1) * WINDOW, 0:256] = out.T.astype(BF16)

    def pool(n):
        first = offset + n * WINDOW
        i = lax.broadcasted_iota(jnp.int32, (WINDOW, WINDOW + 2 * RIM), 0)
        j = lax.broadcasted_iota(jnp.int32, (WINDOW, WINDOW + 2 * RIM), 1) - RIM
        pos = first + j
        member = (j >= i - half) & (j < i + half) & (pos >= 0) & (pos < seq_len)
        member = jnp.where(member, 1.0, 0.0).astype(BF16)
        sums = jnp.dot(member, chan[pl.ds(n * WINDOW, WINDOW + 2 * RIM), :], preferred_element_type=F32)
        t = first + lax.broadcasted_iota(jnp.int32, (WINDOW, 1), 0)
        count = (jnp.minimum(t + half, seq_len) - jnp.maximum(t - half, 0)).astype(F32)
        spread = (sums / count - chan[pl.ds(n * WINDOW + RIM, WINDOW), :].astype(F32)).astype(BF16)
        pooled = jnp.dot(spread, wpool[0], preferred_element_type=F32) * scale[...]
        hid[n * WINDOW : (n + 1) * WINDOW, 256:512] = pooled.astype(BF16)

    def mixers(first, second):
        for n in (first, second):
            pool(n)
            attend(n)

    def partials(first, second):
        both = jnp.concatenate([hid[chunk(first), :], hid[chunk(second), :]], axis=0)
        for d in (2, 1, 3, 0):
            cols = pl.ds(pl.multiple_of(lax.rem(y + d, NY) * feats, feats), feats)
            terms = lax.dot_general(both, wout_abs[cols, :], NT, preferred_element_type=F32).astype(BF16)
            part[d, chunk(first), :] = terms[:WINDOW]
            part[d, chunk(second), :] = terms[WINDOW:]

    def send(first, second):
        for n in (first, second):
            message(part.at[2, chunk(n)], relayed.at[chunk(n)], dev_y(1 if n < 2 else -1), "sum", "via%d" % n).start()
        for n in (first, second):
            got = "sum%d" % (n in (0, 3))
            if n < 2:
                message(part.at[3, chunk(n)], from_next.at[chunk(n)], dev_y(-1), "sum", got).start()
            else:
                message(part.at[1, chunk(n)], from_prev.at[chunk(n)], dev_y(1), "sum", got).start()

    def relay(n):
        at = chunk(n)
        waiting(relayed.at[at], "recv", "via%d" % n)
        mine = part[1 if n < 2 else 3, at, :]
        comb[at, :] = (mine.astype(F32) + relayed[at, :].astype(F32)).astype(BF16)
        got = "sum%d" % (n in (0, 3))
        if n < 2:
            message(comb.at[at], from_prev.at[at], dev_y(1), "sum", got).start()
        else:
            message(comb.at[at], from_next.at[at], dev_y(-1), "sum", got).start()

    with jax.named_scope("mix12"):
        mixers(1, 2)
    with jax.named_scope("out_relay_third"):
        outof.last_near()
        outof.relay_third()
    with jax.named_scope("halo"):
        waiting(kv.at[pl.ds(0, 2 * WINDOW)], "recv", "kv")
        waiting(chan.at[pl.ds(0, 2 * RIM)], "recv", "ch")
    with jax.named_scope("mix03"):
        mixers(0, 3)
    with jax.named_scope("out_last"):
        outof.in_order(wout_abs, NEAR)
        outof.last_far()
        outof.in_order(wout_abs, FAR)
    with jax.named_scope("part12"):
        partials(1, 2)
        send(1, 2)
    with jax.named_scope("part03"):
        partials(0, 3)
        send(0, 3)
    with jax.named_scope("relay12"):
        relay(1)
        relay(2)
    with jax.named_scope("relay03"):
        relay(0)
        relay(3)

    lane = lax.broadcasted_iota(jnp.int32, (WINDOW, 128), 1)

    def settle(p, first, second):
        waiting(from_prev, "recv", "sum%d" % p)
        for k, n in enumerate((first, second)):
            at = chunk(n)
            mix = part[0, at, :].astype(F32) + from_prev[at, :].astype(F32) + from_next[at, :].astype(F32)
            share[at, :] = mix
            one = jnp.sum(mix, axis=1, keepdims=True)
            two = jnp.sum(mix * mix, axis=1, keepdims=True)
            both = jnp.where(lane == 0, one, jnp.where(lane == 1, two, 0.0))
            stats[4 * p, k * 8 : k * 8 + 8, :] = both.T[0:8]
        for d, slot in ((2, 2), (1, 3), (-1, 1)):
            message(stats.at[4 * p], stats.at[4 * p + slot], dev_y(d), "told%d" % p, "told%d" % p).start()

    width = feats * NY
    writes = []

    def finish(p, first, second):
        waiting(stats.at[pl.ds(0, 3)], "recv", "told%d" % p)
        for k, n in enumerate((first, second)):
            at = chunk(n)
            eight = slice(k * 8, k * 8 + 8)
            both = stats[4 * p, eight, :] + stats[4 * p + 1, eight, :]
            both = both + stats[4 * p + 2, eight, :] + stats[4 * p + 3, eight, :]
            both = jnp.concatenate([both] * 16, axis=0).T
            mean = both[:, 0:1] / width
            variance = both[:, 1:2] / width - mean * mean
            normed = (share[at, :] - mean) * lax.rsqrt(variance + epsilon) * gain[...]
            outv[at, :] = normed.astype(BF16)
            writes.append(pltpu.make_async_copy(outv.at[at], out_hbm.at[at], out_sem.at[n]))
            writes[-1].start()

    with jax.named_scope("settle12"):
        settle(0, 1, 2)
    with jax.named_scope("settle03"):
        settle(1, 0, 3)
    with jax.named_scope("finish12"):
        finish(0, 1, 2)
        into.sent()
        outof.sent()
        for ref, name in (
            (toks.at[pl.ds(0, 3)], "tok"), (part.at[pl.ds(0, 3)], "sum"), (kv.at[pl.ds(0, 2 * WINDOW)], "kv"),
            (chan.at[pl.ds(0, 2 * RIM)], "ch"), (stats.at[pl.ds(0, 3)], "told0"), (stats.at[pl.ds(0, 3)], "told1"),
        ):
            waiting(ref, "send", name)
    with jax.named_scope("finish03"):
        finish(1, 0, 3)
        for write in writes:
            write.wait()
    assert len(groups) == SEMAPHORES


SEMAPHORES = 57


def local(tokens, w_query, w_key, w_value, w_pool_in, sink, w_pool, pool_scale, w_out_attn, w_out_pool, out_gain):
    rows, feats = tokens.shape
    hbm = pl.BlockSpec(memory_space=pltpu.HBM)
    lanes_in = 640
    lanes_out = 512
    model = feats * NY
    return pl.pallas_call(
        kernel,
        out_shape=jax.ShapeDtypeStruct((rows, feats), BF16),
        in_specs=[hbm] * 11,
        out_specs=hbm,
        scratch_shapes=[
            pltpu.VMEM((NY, rows, feats), BF16),
            pltpu.VMEM((NX * NC * NZ, 16, lanes_in), BF16),
            pltpu.VMEM((NX * NC * NZ, 16, lanes_out), BF16),
            pltpu.VMEM((model, lanes_in), BF16),
            pltpu.VMEM((model, lanes_out), BF16),
            pltpu.VMEM((rows, 256), BF16),
            pltpu.VMEM((rows + 2 * WINDOW, 128), BF16),
            pltpu.VMEM((rows + 2 * RIM, 256), BF16),
            pltpu.VMEM((rows, lanes_out), BF16),
            pltpu.VMEM((NY, rows, feats), BF16),
            pltpu.VMEM((rows, feats), BF16),
            pltpu.VMEM((rows, feats), BF16),
            pltpu.VMEM((rows, feats), BF16),
            pltpu.VMEM((rows, feats), BF16),
            pltpu.VMEM((rows, feats), F32),
            pltpu.VMEM((2 * NY, 16, 128), F32),
            pltpu.VMEM((16, 64), BF16),
            pltpu.VMEM((16, 64), BF16),
            pltpu.VMEM((1, 4), F32),
            pltpu.VMEM((1, 256, 256), BF16),
            pltpu.VMEM((1, 256), F32),
            pltpu.VMEM((1, 512), F32),
            pltpu.VMEM((rows, feats), BF16),
            pltpu.SemaphoreType.DMA((11,)),
            pltpu.SemaphoreType.DMA((4,)),
            pltpu.SemaphoreType.DMA((SEMAPHORES,)),
        ],
        compiler_params=pltpu.CompilerParams(
            collective_id=0, has_side_effects=True
        ),
    )(
        tokens, w_query, w_key, w_value, w_pool_in, sink.reshape(1, -1), w_pool, pool_scale.reshape(1, -1),
        w_out_attn.T, w_out_pool.T, out_gain.reshape(1, -1),
    )


def solution(mesh):
    finer = Mesh(mesh.devices.reshape(NZ, NX, NC, NY), (*SP, "tp"))
    return jax.shard_map(
        local,
        mesh=finer,
        in_specs=(
            P(SP, "tp"), P(SP, "tp"), P(SP, "tp"), P(SP, "tp"), P(SP, "tp"), P("tp"),
            P("tp", None, None), P("tp"), P("tp", SP), P("tp", SP), P("tp"),
        ),
        out_specs=P(SP, "tp"),
        check_vma=False,
    )
```

```python
import jax
import jax.numpy as jnp
from jax import lax
from jax.experimental import pallas as pl
from jax.experimental.pallas import tpu as pltpu
from jax.sharding import Mesh
from jax.sharding import PartitionSpec as P

HEAD_DIM = 64
WINDOW = 128
RIM = 16
SP = ("sp_0", "sp_1", "sp_2")
MESH = pl.DeviceIdType.MESH
NZ, NX, NC, NY = 16, 4, 2, 4

epsilon = 1e-05
masked_score = -1e30

OWN, NEAR, FAR = 4, (0, 9), (9, 16)
FIRST, LOW, HIGH = (2, 7), (0, 2), (7, 9)
NT = (((1,), (1,)), ((), ()))
TN = (((0,), (0,)), ((), ()))
BF16, F32 = jnp.bfloat16, jnp.float32


def kernel(
    tok_hbm, wq_hbm, wk_hbm, wv_hbm, wc_hbm, sink_hbm, wpool_hbm, scale_hbm, woa_hbm, wop_hbm, gain_hbm,
    out_hbm,
    toks, win, wout, win_abs, wout_abs, query, kv, chan, hid, part, comb, relayed, from_prev, from_next,
    share, stats, wk, wv, sink, wpool, scale, gain, outv, local_sem, out_sem, sems,
):
    z, x, c, y = (lax.axis_index(a) for a in (*SP, "tp"))
    rows, feats = toks.shape[1], toks.shape[2]
    seq_len = rows * NZ * NX * NC
    place = (z * NX + x) * NC + c
    offset = place * rows
    total_places = NZ * NX * NC

    def dev_z(d):
        return {"sp_0": lax.rem(z + (d + NZ), NZ)}

    def dev_x(d):
        return {"sp_1": lax.rem(x + (d + NX), NX)}

    def dev_y(d):
        return {"tp": lax.rem(y + (d + NY), NY)}

    dev_c = {"sp_2": 1 - c}

    def dev_sp(d):
        s = lax.rem(place + (d + total_places), total_places)
        return {
            "sp_0": lax.div(s, NX * NC),
            "sp_1": lax.rem(lax.div(s, NC), NX),
            "sp_2": lax.rem(s, NC),
        }

    peers = [dev_z(d) for d in (4, -4, 3, -3, 2, -2, 1, -1)]
    peers += [dev_y(2), dev_x(2), dev_sp(1), dev_sp(-1), dev_x(1), dev_x(-1), dev_y(1), dev_y(-1), dev_c]
    barrier = pltpu.get_barrier_semaphore()
    for peer in peers:
        pl.semaphore_signal(barrier, inc=1, device_id=peer, device_id_type=MESH)

    mine_in, mine_out = win.at[OWN], wout.at[OWN]
    pairs = (
        (wk_hbm, wk), (wv_hbm, wv), (wq_hbm, mine_in.at[:, pl.ds(0, 256)]), (wc_hbm, mine_in.at[:, pl.ds(384, 256)]),
        (tok_hbm, toks.at[0]), (woa_hbm, mine_out.at[:, pl.ds(0, 256)]), (wop_hbm, mine_out.at[:, pl.ds(256, 256)]),
        (wpool_hbm, wpool), (scale_hbm, scale), (gain_hbm, gain), (sink_hbm, sink),
    )
    loads = [pltpu.make_async_copy(a, b, local_sem.at[k]) for k, (a, b) in enumerate(pairs)]
    for load in loads:
        load.start()

    with jax.named_scope("entry"):
        loads[0].wait()
        loads[1].wait()
        win[OWN, :, 256:384] = jnp.concatenate([wk[...], wv[...]], axis=1)
        for load in loads[2:]:
            load.wait()
        pl.semaphore_wait(barrier, len(peers))

    groups = {}

    def message(src, dst, device, sent, got):
        for key in (("send", sent), ("recv", got)):
            groups.setdefault(key, len(groups))
        return pltpu.make_async_remote_copy(
            src_ref=src, dst_ref=dst, send_sem=sems.at[groups["send", sent]], recv_sem=sems.at[groups["recv", got]],
            device_id=device, device_id_type=MESH,
        )

    def waiting(ref, kind, name):
        sem = sems.at[groups[kind, name]]
        copy = pltpu.make_async_remote_copy(
            src_ref=ref, dst_ref=ref, send_sem=sem, recv_sem=sem, device_id=dev_c, device_id_type=MESH
        )
        if kind == "send":
            copy.wait_send()
        else:
            copy.wait_recv()

    class Gather:
        def __init__(self, w, name):
            self.w, self.name = w, name

        def at(self, r, k, lo, hi):
            return self.w.at[pl.ds((r * NC + k) * NZ + lo, hi - lo)]

        def send(self, src, dst, device, got):
            message(src, dst, device, self.name, self.name + got).start()

        def wait(self, slots, got):
            waiting(self.w.at[pl.ds(0, slots)], "recv", self.name + got)

        def near(self):
            for d in (1, -1, 2, -2, 4, -4, 3, -3):
                p = (4 - d) % NZ
                got = {4: "m4", -4: "p4", 3: "n3", -3: "n3"}.get(d, "n1")
                self.send(self.at(0, 0, OWN, OWN + 1), self.at(0, 0, p, p + 1), dev_z(d), got)

        def far(self):
            self.wait(1, "m4")
            for e in (4, 3, 2, 1):
                self.send(self.at(0, 0, 0, 1), self.at(0, 0, 16 - e, 17 - e), dev_z(e), "far")
            self.wait(1, "p4")
            for e in (3, 2, 1):
                self.send(self.at(0, 0, 8, 9), self.at(0, 0, 8 + e, 9 + e), dev_z(-e), "far")

        def along_x(self, span):
            self.send(self.at(0, 0, *span), self.at(3, 0, *span), dev_x(1), "xp%d" % span[0])
            self.send(self.at(0, 0, *span), self.at(1, 0, *span), dev_x(-1), "xm%d" % span[0])

        def wait_x(self, r, span):
            self.wait(span[1] - span[0], ("xp%d" if r == 3 else "xm%d") % span[0])

        def relay_x(self, r, span):
            part = "near" if span[0] < 9 else "rest"
            self.send(self.at(r, 0, *span), self.at(2, 0, *span), dev_x(1 if r == 3 else -1), "x2" + part)

        def across(self, r, span):
            part = "near" if span[0] < 9 else "rest"
            self.send(self.at(r, 0, *span), self.at(r, 1, *span), dev_c, "c" + part)

        def first(self):
            self.wait(4, "n1")
            self.along_x(FIRST)

        def second(self):
            self.wait(2, "n3")
            self.along_x(LOW)
            self.along_x(HIGH)
            self.across(0, NEAR)

        def third(self):
            self.wait(7, "far")
            self.along_x(FAR)
            self.across(0, FAR)

        def relay_first(self):
            self.wait_x(3, FIRST)
            self.relay_x(3, (2, 5))
            self.wait_x(1, FIRST)
            self.relay_x(1, (5, 7))

        def relay_second(self):
            self.wait_x(3, LOW)
            self.relay_x(3, LOW)
            self.wait_x(1, HIGH)
            self.relay_x(1, HIGH)
            self.wait_x(3, HIGH)
            self.across(3, NEAR)
            self.wait_x(1, LOW)
            self.across(1, NEAR)

        def relay_third(self):
            self.wait_x(3, FAR)
            self.relay_x(3, (9, 12))
            self.across(3, FAR)
            self.wait_x(1, FAR)
            self.relay_x(1, (12, 16))
            self.across(1, FAR)

        def last_near(self):
            self.wait(9, "x2near")
            self.across(2, NEAR)

        def last_far(self):
            self.wait(7, "x2rest")
            self.across(2, FAR)

        def in_order(self, dest, span):
            w = self.w
            self.wait(NX * (span[1] - span[0]), "cnear" if span[0] < 9 else "crest")

            def one(p, carry):
                base = lax.rem(z + p + (NZ - 4), NZ) * (NX * NC * 16)
                for r in range(NX):
                    for k in range(NC):
                        at = base + lax.rem(x + r, NX) * (NC * 16) + lax.rem(c + k, NC) * 16
                        dest[pl.ds(pl.multiple_of(at, 16), 16), :] = w[(r * NC + k) * NZ + p]
                return carry

            lax.fori_loop(*span, one, 0)

        def sent(self):
            waiting(self.w.at[pl.ds(0, 127)], "send", self.name)

    into = Gather(win, "in")
    outof = Gather(wout, "out")

    def chunk(b):
        return pl.ds(b * WINDOW, WINDOW)

    def tokens_to(slot, b, src, d, got):
        message(toks.at[src, chunk(b)], toks.at[slot, chunk(b)], dev_y(d), "tok", got).start()

    def tokens_relay(b):
        waiting(toks.at[0, chunk(0)], "recv", "tok%d" % b)
        if b < 2:
            tokens_to(2, b, 3, 1, "tok")
        else:
            tokens_to(2, b, 1, -1, "tok")

    with jax.named_scope("near"):
        into.near()
        for b in (0, 1):
            tokens_to(3, b, 0, 1, "tok%d" % b)
            tokens_to(1, b + 2, 0, -1, "tok%d" % (b + 2))
        for b in (0, 1):
            tokens_to(3, b + 2, 0, 1, "tok")
            tokens_to(1, b, 0, -1, "tok")
    with jax.named_scope("in_first"):
        into.first()
    with jax.named_scope("in_far"):
        into.far()
        outof.near()
    with jax.named_scope("in_second"):
        into.second()
    with jax.named_scope("tok_relay_a"):
        tokens_relay(0)
        tokens_relay(2)
    with jax.named_scope("in_relay_first"):
        into.relay_first()
    with jax.named_scope("tok_relay_b"):
        tokens_relay(1)
        tokens_relay(3)
    with jax.named_scope("in_relay_second"):
        into.relay_second()
    with jax.named_scope("in_third"):
        into.third()
    with jax.named_scope("in_last_near"):
        into.last_near()
    with jax.named_scope("out_first"):
        outof.first()
    with jax.named_scope("out_far"):
        outof.far()
    with jax.named_scope("out_second"):
        outof.second()
    with jax.named_scope("in_relay_third"):
        into.relay_third()
    with jax.named_scope("in_order_near"):
        into.in_order(win_abs, NEAR)
    with jax.named_scope("out_relay_first"):
        outof.relay_first()
        outof.relay_second()
    with jax.named_scope("out_third"):
        outof.third()
    with jax.named_scope("in_last_far"):
        into.last_far()
    with jax.named_scope("in_order_far"):
        into.in_order(win_abs, FAR)
    with jax.named_scope("tok_done"):
        waiting(toks.at[pl.ds(0, 2)], "recv", "tok")

    def project(lo, hi):
        acc = jnp.zeros((rows, hi - lo), F32)
        for r in range(NY):
            depth = pl.ds(pl.multiple_of(lax.rem(y + r, NY) * feats, feats), feats)
            acc = acc + jnp.dot(toks[r], win_abs[depth, lo:hi], preferred_element_type=F32)
        return acc

    own_kv, own_ch = (kv, WINDOW, "kv"), (chan, RIM, "ch")

    def to_neighbours(ref, size, name):
        message(ref.at[pl.ds(rows, size)], ref.at[pl.ds(0, size)], dev_sp(1), name, name).start()
        message(ref.at[pl.ds(size, size)], ref.at[pl.ds(size + rows, size)], dev_sp(-1), name, name).start()

    with jax.named_scope("project"):
        kv[pl.ds(WINDOW, rows), :] = project(256, 384).astype(BF16)
        chan[pl.ds(RIM, rows), :] = project(384, 640).astype(BF16)
        query[...] = (project(0, 256) * HEAD_DIM ** (-0.5)).astype(BF16)
        to_neighbours(*own_kv)
        to_neighbours(*own_ch)
    with jax.named_scope("out_relay_third"):
        outof.relay_third()
        outof.last_near()

    half = lax.shift_left(jnp.int32(1), y.astype(jnp.int32))
    sinks = jnp.concatenate([jnp.broadcast_to(sink[0:1, h : h + 1], (1, WINDOW)) for h in range(4)], axis=1)

    def attend(n):
        first = offset + n * WINDOW
        band = kv[pl.ds(n * WINDOW, 3 * WINDOW), :]
        keys, values = band[:, :HEAD_DIM], band[:, HEAD_DIM:]
        block = query[n * WINDOW : (n + 1) * WINDOW, :]
        stacked = jnp.concatenate([block[:, h * HEAD_DIM : (h + 1) * HEAD_DIM] for h in range(4)], axis=0)
        scores = lax.dot_general(keys, stacked, NT, preferred_element_type=F32)
        j = lax.broadcasted_iota(jnp.int32, (WINDOW, 4 * WINDOW), 0)
        i = lax.rem(lax.broadcasted_iota(jnp.int32, (WINDOW, 4 * WINDOW), 1), WINDOW)
        before = jnp.where((j >= i) & (first > 0), scores[:WINDOW], masked_score)
        here = scores[WINDOW : 2 * WINDOW]
        after = jnp.where((j <= i) & (first + WINDOW < seq_len), scores[2 * WINDOW :], masked_score)
        top = jnp.max(jnp.maximum(jnp.maximum(before, here), after), axis=0, keepdims=True)
        top = jnp.maximum(top, sinks)
        before, here, after = jnp.exp(before - top), jnp.exp(here - top), jnp.exp(after - top)
        total = jnp.sum(before + here + after, axis=0, keepdims=True) + jnp.exp(sinks - top)
        inverse = 1.0 / total
        probs = jnp.concatenate([(r * inverse).astype(BF16) for r in (before, here, after)], axis=0)
        out = lax.dot_general(values, probs, TN, preferred_element_type=F32)
        out = jnp.concatenate([out[:, h * WINDOW : (h + 1) * WINDOW] for h in range(4)], axis=0)
        hid[n * WINDOW : (n + 1) * WINDOW, 0:256] = out.T.astype(BF16)

    def pool(n):
        first = offset + n * WINDOW
        i = lax.broadcasted_iota(jnp.int32, (WINDOW, WINDOW + 2 * RIM), 0)
        j = lax.broadcasted_iota(jnp.int32, (WINDOW, WINDOW + 2 * RIM), 1) - RIM
        pos = first + j
        member = (j >= i - half) & (j < i + half) & (pos >= 0) & (pos < seq_len)
        member = jnp.where(member, 1.0, 0.0).astype(BF16)
        sums = jnp.dot(member, chan[pl.ds(n * WINDOW, WINDOW + 2 * RIM), :], preferred_element_type=F32)
        t = first + lax.broadcasted_iota(jnp.int32, (WINDOW, 1), 0)
        count = (jnp.minimum(t + half, seq_len) - jnp.maximum(t - half, 0)).astype(F32)
        spread = (sums / count - chan[pl.ds(n * WINDOW + RIM, WINDOW), :].astype(F32)).astype(BF16)
        pooled = jnp.dot(spread, wpool[0], preferred_element_type=F32) * scale[...]
        hid[n * WINDOW : (n + 1) * WINDOW, 256:512] = pooled.astype(BF16)

    def mixers(first, second):
        for n in (first, second):
            pool(n)
            attend(n)

    def partials(p, first, second):
        both = jnp.concatenate([hid[chunk(first), :], hid[chunk(second), :]], axis=0)
        for d in (2, 3, 1, 0):
            cols = pl.ds(pl.multiple_of(lax.rem(y + d, NY) * feats, feats), feats)
            terms = lax.dot_general(both, wout_abs[cols, :], NT, preferred_element_type=F32).astype(BF16)
            part[d, chunk(first), :] = terms[:WINDOW]
            part[d, chunk(second), :] = terms[WINDOW:]
        for n in (first, second):
            target = dev_y(1 if n < 2 else -1)
            message(part.at[2, chunk(n)], relayed.at[chunk(n)], target, "sum", "via%d" % n).start()
        for n in (first, second):
            if n < 2:
                message(part.at[3, chunk(n)], from_next.at[chunk(n)], dev_y(-1), "sum", "sum%d" % p).start()
            else:
                message(part.at[1, chunk(n)], from_prev.at[chunk(n)], dev_y(1), "sum", "sum%d" % p).start()

    def relay(n):
        at = chunk(n)
        waiting(relayed.at[at], "recv", "via%d" % n)
        mine = part[1 if n < 2 else 3, at, :]
        comb[at, :] = (mine.astype(F32) + relayed[at, :].astype(F32)).astype(BF16)
        got = "sum%d" % (n in (0, 3))
        if n < 2:
            message(comb.at[at], from_prev.at[at], dev_y(1), "sum", got).start()
        else:
            message(comb.at[at], from_next.at[at], dev_y(-1), "sum", got).start()

    with jax.named_scope("mix12"):
        mixers(1, 2)
    with jax.named_scope("out_order_near"):
        outof.in_order(wout_abs, NEAR)
    with jax.named_scope("out_last_far"):
        outof.last_far()
    with jax.named_scope("halo"):
        waiting(kv.at[pl.ds(0, 2 * WINDOW)], "recv", "kv")
        waiting(chan.at[pl.ds(0, 2 * RIM)], "recv", "ch")
    with jax.named_scope("mix03"):
        mixers(0, 3)
    with jax.named_scope("out_last"):
        outof.in_order(wout_abs, FAR)
    with jax.named_scope("part12"):
        partials(0, 1, 2)
    with jax.named_scope("part03"):
        partials(1, 0, 3)
    with jax.named_scope("relay12"):
        relay(1)
        relay(2)
    with jax.named_scope("relay03"):
        relay(0)
        relay(3)

    lane = lax.broadcasted_iota(jnp.int32, (WINDOW, 128), 1)

    def settle(p, first, second):
        waiting(from_prev, "recv", "sum%d" % p)
        for k, n in enumerate((first, second)):
            at = chunk(n)
            mix = part[0, at, :].astype(F32) + from_prev[at, :].astype(F32) + from_next[at, :].astype(F32)
            share[at, :] = mix
            one = jnp.sum(mix, axis=1, keepdims=True)
            two = jnp.sum(mix * mix, axis=1, keepdims=True)
            both = jnp.where(lane == 0, one, jnp.where(lane == 1, two, 0.0))
            stats[4 * p, k * 8 : k * 8 + 8, :] = both.T[0:8]
        for d, slot in ((2, 2), (1, 3), (-1, 1)):
            message(stats.at[4 * p], stats.at[4 * p + slot], dev_y(d), "told%d" % p, "told%d" % p).start()

    width = feats * NY
    writes = []

    def finish(p, first, second):
        waiting(stats.at[pl.ds(0, 3)], "recv", "told%d" % p)
        for k, n in enumerate((first, second)):
            at = chunk(n)
            eight = slice(k * 8, k * 8 + 8)
            both = stats[4 * p, eight, :] + stats[4 * p + 1, eight, :]
            both = both + stats[4 * p + 2, eight, :] + stats[4 * p + 3, eight, :]
            both = jnp.concatenate([both] * 16, axis=0).T
            mean = both[:, 0:1] / width
            variance = both[:, 1:2] / width - mean * mean
            normed = (share[at, :] - mean) * lax.rsqrt(variance + epsilon) * gain[...]
            outv[at, :] = normed.astype(BF16)
            writes.append(pltpu.make_async_copy(outv.at[at], out_hbm.at[at], out_sem.at[n]))
            writes[-1].start()

    with jax.named_scope("settle12"):
        settle(0, 1, 2)
    with jax.named_scope("settle03"):
        settle(1, 0, 3)
    with jax.named_scope("finish12"):
        finish(0, 1, 2)
        into.sent()
        outof.sent()
        for ref, name in (
            (toks.at[pl.ds(0, 3)], "tok"), (part.at[pl.ds(0, 3)], "sum"), (kv.at[pl.ds(0, 2 * WINDOW)], "kv"),
            (chan.at[pl.ds(0, 2 * RIM)], "ch"), (stats.at[pl.ds(0, 3)], "told0"), (stats.at[pl.ds(0, 3)], "told1"),
        ):
            waiting(ref, "send", name)
    with jax.named_scope("finish03"):
        finish(1, 0, 3)
        for write in writes:
            write.wait()
    assert len(groups) == SEMAPHORES


SEMAPHORES = 57


def local(tokens, w_query, w_key, w_value, w_pool_in, sink, w_pool, pool_scale, w_out_attn, w_out_pool, out_gain):
    rows, feats = tokens.shape
    hbm = pl.BlockSpec(memory_space=pltpu.HBM)
    lanes_in = 640
    lanes_out = 512
    model = feats * NY
    return pl.pallas_call(
        kernel,
        out_shape=jax.ShapeDtypeStruct((rows, feats), BF16),
        in_specs=[hbm] * 11,
        out_specs=hbm,
        scratch_shapes=[
            pltpu.VMEM((NY, rows, feats), BF16),
            pltpu.VMEM((NX * NC * NZ, 16, lanes_in), BF16),
            pltpu.VMEM((NX * NC * NZ, 16, lanes_out), BF16),
            pltpu.VMEM((model, lanes_in), BF16),
            pltpu.VMEM((model, lanes_out), BF16),
            pltpu.VMEM((rows, 256), BF16),
            pltpu.VMEM((rows + 2 * WINDOW, 128), BF16),
            pltpu.VMEM((rows + 2 * RIM, 256), BF16),
            pltpu.VMEM((rows, lanes_out), BF16),
            pltpu.VMEM((NY, rows, feats), BF16),
            pltpu.VMEM((rows, feats), BF16),
            pltpu.VMEM((rows, feats), BF16),
            pltpu.VMEM((rows, feats), BF16),
            pltpu.VMEM((rows, feats), BF16),
            pltpu.VMEM((rows, feats), F32),
            pltpu.VMEM((2 * NY, 16, 128), F32),
            pltpu.VMEM((16, 64), BF16),
            pltpu.VMEM((16, 64), BF16),
            pltpu.VMEM((1, 4), F32),
            pltpu.VMEM((1, 256, 256), BF16),
            pltpu.VMEM((1, 256), F32),
            pltpu.VMEM((1, 512), F32),
            pltpu.VMEM((rows, feats), BF16),
            pltpu.SemaphoreType.DMA((11,)),
            pltpu.SemaphoreType.DMA((4,)),
            pltpu.SemaphoreType.DMA((SEMAPHORES,)),
        ],
        compiler_params=pltpu.CompilerParams(
            collective_id=0, has_side_effects=True
        ),
    )(
        tokens, w_query, w_key, w_value, w_pool_in, sink.reshape(1, -1), w_pool, pool_scale.reshape(1, -1),
        w_out_attn.T, w_out_pool.T, out_gain.reshape(1, -1),
    )


def solution(mesh):
    finer = Mesh(mesh.devices.reshape(NZ, NX, NC, NY), (*SP, "tp"))
    return jax.shard_map(
        local,
        mesh=finer,
        in_specs=(
            P(SP, "tp"), P(SP, "tp"), P(SP, "tp"), P(SP, "tp"), P(SP, "tp"), P("tp"),
            P("tp", None, None), P("tp"), P("tp", SP), P("tp", SP), P("tp"),
        ),
        out_specs=P(SP, "tp"),
        check_vma=False,
    )
```

```python
import jax
import jax.numpy as jnp
from jax import lax
from jax.experimental import pallas as pl
from jax.experimental.pallas import tpu as pltpu
from jax.sharding import Mesh
from jax.sharding import PartitionSpec as P

HEAD_DIM = 64
WINDOW = 128
RIM = 16
SP = ("sp_0", "sp_1", "sp_2")
MESH = pl.DeviceIdType.MESH
NZ, NX, NC, NY = 16, 4, 2, 4

epsilon = 1e-05
masked_score = -1e30

OWN, NEAR, FAR = 4, (0, 9), (9, 16)
FIRST, SECOND, THIRD = ((2, 5), (5, 7)), ((0, 2), (7, 9)), ((9, 12), (12, 16))
NT = (((1,), (1,)), ((), ()))
TN = (((0,), (0,)), ((), ()))
BF16, F32 = jnp.bfloat16, jnp.float32


def kernel(
    tok_hbm, wq_hbm, wk_hbm, wv_hbm, wc_hbm, sink_hbm, wpool_hbm, scale_hbm, woa_hbm, wop_hbm, gain_hbm,
    out_hbm,
    toks, win, wout, win_abs, wout_abs, query, kv, chan, hid, part, comb, relayed, from_prev, from_next,
    share, stats, turned_toks, acc, wk, wv, sink, wpool, scale, gain, outv, local_sem, out_sem, sems,
):
    z, x, c, y = (lax.axis_index(a) for a in (*SP, "tp"))
    rows, feats = toks.shape[1], toks.shape[2]
    seq_len = rows * NZ * NX * NC
    place = (z * NX + x) * NC + c
    offset = place * rows
    total_places = NZ * NX * NC

    def dev_z(d):
        return {"sp_0": lax.rem(z + (d + NZ), NZ)}

    def dev_x(d):
        return {"sp_1": lax.rem(x + (d + NX), NX)}

    def dev_y(d):
        return {"tp": lax.rem(y + (d + NY), NY)}

    dev_c = {"sp_2": 1 - c}

    def dev_sp(d):
        s = lax.rem(place + (d + total_places), total_places)
        return {
            "sp_0": lax.div(s, NX * NC),
            "sp_1": lax.rem(lax.div(s, NC), NX),
            "sp_2": lax.rem(s, NC),
        }

    peers = [dev_z(d) for d in (4, -4, 3, -3, 2, -2, 1, -1)]
    peers += [dev_y(2), dev_sp(1), dev_sp(-1), dev_x(1), dev_x(-1), dev_y(1), dev_y(-1), dev_c]
    mine_in, mine_out = win.at[OWN], wout.at[OWN]
    pairs = (
        (wk_hbm, wk), (wv_hbm, wv), (wq_hbm, mine_in.at[:, pl.ds(0, 256)]), (wc_hbm, mine_in.at[:, pl.ds(384, 256)]),
        (woa_hbm, mine_out.at[:, pl.ds(0, 256)]), (wop_hbm, mine_out.at[:, pl.ds(256, 256)]), (tok_hbm, toks.at[0]),
        (wpool_hbm, wpool), (scale_hbm, scale), (gain_hbm, gain), (sink_hbm, sink),
    )
    loads = [pltpu.make_async_copy(a, b, local_sem.at[k]) for k, (a, b) in enumerate(pairs)]
    for load in loads:
        load.start()

    barrier = pltpu.get_barrier_semaphore()
    for peer in peers:
        pl.semaphore_signal(barrier, inc=1, device_id=peer, device_id_type=MESH)

    with jax.named_scope("entry"):
        loads[0].wait()
        loads[1].wait()
        win[OWN, :, 256:384] = jnp.concatenate([wk[...], wv[...]], axis=1)
        for load in loads[2:6]:
            load.wait()
        pl.semaphore_wait(barrier, len(peers))

    groups = {}

    def message(src, dst, device, sent, got):
        for key in (("send", sent), ("recv", got)):
            groups.setdefault(key, len(groups))
        return pltpu.make_async_remote_copy(
            src_ref=src, dst_ref=dst, send_sem=sems.at[groups["send", sent]], recv_sem=sems.at[groups["recv", got]],
            device_id=device, device_id_type=MESH,
        )

    def waiting(ref, kind, name):
        sem = sems.at[groups[kind, name]]
        copy = pltpu.make_async_remote_copy(
            src_ref=ref, dst_ref=ref, send_sem=sem, recv_sem=sem, device_id=dev_c, device_id_type=MESH
        )
        if kind == "send":
            copy.wait_send()
        else:
            copy.wait_recv()

    class Gather:
        def __init__(self, w, name):
            self.w, self.name = w, name

        def at(self, r, k, lo, hi):
            return self.w.at[pl.ds((r * NC + k) * NZ + lo, hi - lo)]

        def send(self, src, dst, device, got):
            message(src, dst, device, self.name, self.name + got).start()

        def wait(self, slots, got):
            waiting(self.w.at[pl.ds(0, slots)], "recv", self.name + got)

        def near(self):
            for d in (1, -1, 2, -2, 4, -4, 3, -3):
                p = (4 - d) % NZ
                got = {4: "m4", -4: "p4", 3: "n3", -3: "n3"}.get(d, "n1")
                self.send(self.at(0, 0, OWN, OWN + 1), self.at(0, 0, p, p + 1), dev_z(d), got)

        def far(self):
            self.wait(1, "m4")
            for e in (4, 3, 2, 1):
                self.send(self.at(0, 0, 0, 1), self.at(0, 0, 16 - e, 17 - e), dev_z(e), "far")
            self.wait(1, "p4")
            for e in (3, 2, 1):
                self.send(self.at(0, 0, 8, 9), self.at(0, 0, 8 + e, 9 + e), dev_z(-e), "far")

        def along_x(self, stage):
            up, down = stage
            others = "o%d" % (stage is THIRD)
            self.send(self.at(0, 0, *up), self.at(3, 0, *up), dev_x(1), "x%d" % up[0])
            self.send(self.at(0, 0, *down), self.at(1, 0, *down), dev_x(-1), "x%d" % down[0])
            self.send(self.at(0, 0, *down), self.at(3, 0, *down), dev_x(1), others)
            self.send(self.at(0, 0, *up), self.at(1, 0, *up), dev_x(-1), others)

        def relay_x(self, stage):
            part = "rest" if stage is THIRD else "near"
            for r, d, span in ((3, 1, stage[0]), (1, -1, stage[1])):
                self.wait(span[1] - span[0], "x%d" % span[0])
                self.send(self.at(r, 0, *span), self.at(2, 0, *span), dev_x(d), "x2" + part)

        def across(self, r, span):
            part = "near" if span[0] < 9 else "rest"
            self.send(self.at(r, 0, *span), self.at(r, 1, *span), dev_c, "c" + part)

        def first(self):
            self.wait(4, "n1")
            self.along_x(FIRST)

        def second(self):
            self.wait(2, "n3")
            self.along_x(SECOND)
            self.across(0, NEAR)

        def third(self):
            self.wait(7, "far")
            self.along_x(THIRD)
            self.across(0, FAR)

        def others_near(self):
            self.wait(9, "o0")
            self.across(3, NEAR)
            self.across(1, NEAR)

        def others_far(self):
            self.wait(7, "o1")
            self.across(3, FAR)
            self.across(1, FAR)

        def last_near(self):
            self.wait(9, "x2near")
            self.across(2, NEAR)

        def last_far(self):
            self.wait(7, "x2rest")
            self.across(2, FAR)

        def in_order(self, dest, span, turned):
            w = self.w
            self.wait(NX * (span[1] - span[0]), "cnear" if span[0] < 9 else "crest")

            def one(p, carry):
                base = (lax.rem(z + p + (NZ - 4), NZ) if turned else p) * (NX * NC * 16)
                for r in range(NX):
                    for k in range(NC):
                        at = base + lax.rem(x + r, NX) * (NC * 16) + lax.rem(c + k, NC) * 16
                        dest[pl.ds(pl.multiple_of(at, 16), 16), :] = w[(r * NC + k) * NZ + p]
                return carry

            lax.fori_loop(*span, one, 0)

        def sent(self):
            waiting(self.w.at[pl.ds(0, 127)], "send", self.name)

    into = Gather(win, "in")
    outof = Gather(wout, "out")

    def chunk(b):
        return pl.ds(b * WINDOW, WINDOW)

    def tokens_to(slot, b, src, d, got):
        message(toks.at[src, chunk(b)], toks.at[slot, chunk(b)], dev_y(d), "tok", got).start()

    def tokens_relay(b):
        waiting(toks.at[0, chunk(0)], "recv", "tok%d" % b)
        if b < 2:
            tokens_to(2, b, 3, 1, "tok")
        else:
            tokens_to(2, b, 1, -1, "tok")

    with jax.named_scope("near"):
        into.near()
        loads[6].wait()
        for b in (0, 1):
            tokens_to(3, b, 0, 1, "tok%d" % b)
            tokens_to(1, b + 2, 0, -1, "tok%d" % (b + 2))
        for b in (0, 1):
            tokens_to(3, b + 2, 0, 1, "tok")
            tokens_to(1, b, 0, -1, "tok")
    with jax.named_scope("in_first"):
        into.first()
    with jax.named_scope("in_far"):
        into.far()
        outof.near()
        for load in loads[7:]:
            load.wait()
    with jax.named_scope("in_second"):
        into.second()
    with jax.named_scope("tok_relay_a"):
        tokens_relay(0)
        tokens_relay(2)
    with jax.named_scope("in_relay_first"):
        into.relay_x(FIRST)
    with jax.named_scope("tok_relay_b"):
        tokens_relay(1)
        tokens_relay(3)
    with jax.named_scope("in_relay_second"):
        into.relay_x(SECOND)
    with jax.named_scope("in_third"):
        into.third()
    with jax.named_scope("in_others_near"):
        into.others_near()
    with jax.named_scope("out_far"):
        outof.far()
    with jax.named_scope("out_first"):
        outof.first()
    with jax.named_scope("in_last_near"):
        into.last_near()
    with jax.named_scope("in_relay_third"):
        into.relay_x(THIRD)
    with jax.named_scope("out_second"):
        outof.second()
    with jax.named_scope("in_order_near"):
        into.in_order(win_abs, NEAR, False)
    with jax.named_scope("in_others_far"):
        into.others_far()
    with jax.named_scope("out_relay_first"):
        outof.relay_x(FIRST)
    with jax.named_scope("out_third"):
        outof.third()
    with jax.named_scope("in_last_far"):
        into.last_far()
    with jax.named_scope("tok_done"):
        waiting(toks.at[pl.ds(0, 2)], "recv", "tok")
        for p in range(NZ):
            at = lax.rem(z + (p + NZ - 4), NZ)
            per = feats // 128
            r = lax.rem(lax.div(at, per) + (NY - y), NY)
            cols = pl.ds(pl.multiple_of(lax.rem(at, per) * 128, 128), 128)
            turned_toks[:, p * 128 : (p + 1) * 128] = toks[r, :, cols]

    parts = ((256, 384), (384, 640), (0, 256))
    with jax.named_scope("project_near"):
        depth = slice(NEAR[0] * 128, NEAR[1] * 128)
        for lo, hi in parts:
            acc[:, lo:hi] = jnp.dot(turned_toks[:, depth], win_abs[depth, lo:hi], preferred_element_type=F32)
    with jax.named_scope("out_relay_second"):
        outof.relay_x(SECOND)
        outof.others_near()
    with jax.named_scope("in_order_far"):
        into.in_order(win_abs, FAR, False)
    with jax.named_scope("out_relay_third"):
        outof.relay_x(THIRD)

    def project(lo, hi):
        depth = slice(FAR[0] * 128, FAR[1] * 128)
        return acc[:, lo:hi] + jnp.dot(turned_toks[:, depth], win_abs[depth, lo:hi], preferred_element_type=F32)

    own_kv, own_ch = (kv, WINDOW, "kv"), (chan, RIM, "ch")

    def to_neighbours(ref, size, name):
        message(ref.at[pl.ds(rows, size)], ref.at[pl.ds(0, size)], dev_sp(1), name, name).start()
        message(ref.at[pl.ds(size, size)], ref.at[pl.ds(size + rows, size)], dev_sp(-1), name, name).start()

    with jax.named_scope("project"):
        kv[pl.ds(WINDOW, rows), :] = project(256, 384).astype(BF16)
        chan[pl.ds(RIM, rows), :] = project(384, 640).astype(BF16)
        query[...] = (project(0, 256) * HEAD_DIM ** (-0.5)).astype(BF16)
        to_neighbours(*own_kv)
        to_neighbours(*own_ch)
    with jax.named_scope("out_last_near"):
        outof.last_near()
        outof.others_far()

    half = lax.shift_left(jnp.int32(1), y.astype(jnp.int32))
    sinks = jnp.concatenate([jnp.broadcast_to(sink[0:1, h : h + 1], (1, WINDOW)) for h in range(4)], axis=1)

    def attend(n):
        first = offset + n * WINDOW
        band = kv[pl.ds(n * WINDOW, 3 * WINDOW), :]
        keys, values = band[:, :HEAD_DIM], band[:, HEAD_DIM:]
        block = query[n * WINDOW : (n + 1) * WINDOW, :]
        stacked = jnp.concatenate([block[:, h * HEAD_DIM : (h + 1) * HEAD_DIM] for h in range(4)], axis=0)
        scores = lax.dot_general(keys, stacked, NT, preferred_element_type=F32)
        j = lax.broadcasted_iota(jnp.int32, (WINDOW, 4 * WINDOW), 0)
        i = lax.rem(lax.broadcasted_iota(jnp.int32, (WINDOW, 4 * WINDOW), 1), WINDOW)
        before = jnp.where((j >= i) & (first > 0), scores[:WINDOW], masked_score)
        here = scores[WINDOW : 2 * WINDOW]
        after = jnp.where((j <= i) & (first + WINDOW < seq_len), scores[2 * WINDOW :], masked_score)
        top = jnp.max(jnp.maximum(jnp.maximum(before, here), after), axis=0, keepdims=True)
        top = jnp.maximum(top, sinks)
        before, here, after = jnp.exp(before - top), jnp.exp(here - top), jnp.exp(after - top)
        total = jnp.sum(before + here + after, axis=0, keepdims=True) + jnp.exp(sinks - top)
        inverse = 1.0 / total
        probs = jnp.concatenate([(r * inverse).astype(BF16) for r in (before, here, after)], axis=0)
        out = lax.dot_general(values, probs, TN, preferred_element_type=F32)
        out = jnp.concatenate([out[:, h * WINDOW : (h + 1) * WINDOW] for h in range(4)], axis=0)
        hid[n * WINDOW : (n + 1) * WINDOW, 0:256] = out.T.astype(BF16)

    def pool(n):
        first = offset + n * WINDOW
        i = lax.broadcasted_iota(jnp.int32, (WINDOW, WINDOW + 2 * RIM), 0)
        j = lax.broadcasted_iota(jnp.int32, (WINDOW, WINDOW + 2 * RIM), 1) - RIM
        pos = first + j
        member = (j >= i - half) & (j < i + half) & (pos >= 0) & (pos < seq_len)
        member = jnp.where(member, 1.0, 0.0).astype(BF16)
        sums = jnp.dot(member, chan[pl.ds(n * WINDOW, WINDOW + 2 * RIM), :], preferred_element_type=F32)
        t = first + lax.broadcasted_iota(jnp.int32, (WINDOW, 1), 0)
        count = (jnp.minimum(t + half, seq_len) - jnp.maximum(t - half, 0)).astype(F32)
        spread = (sums / count - chan[pl.ds(n * WINDOW + RIM, WINDOW), :].astype(F32)).astype(BF16)
        pooled = jnp.dot(spread, wpool[0], preferred_element_type=F32) * scale[...]
        hid[n * WINDOW : (n + 1) * WINDOW, 256:512] = pooled.astype(BF16)

    def mixers(*which):
        for n in which:
            pool(n)
            attend(n)

    def partials(p, first, second):
        both = jnp.concatenate([hid[chunk(first), :], hid[chunk(second), :]], axis=0)
        for d in (2, 3, 1, 0):
            cols = pl.ds(pl.multiple_of(lax.rem(y + d, NY) * feats, feats), feats)
            terms = lax.dot_general(both, wout_abs[cols, :], NT, preferred_element_type=F32).astype(BF16)
            part[d, chunk(first), :] = terms[:WINDOW]
            part[d, chunk(second), :] = terms[WINDOW:]
        for n in (first, second):
            target = dev_y(1 if n < 2 else -1)
            message(part.at[2, chunk(n)], relayed.at[chunk(n)], target, "sum", "via%d" % n).start()
        for n in (first, second):
            if n < 2:
                message(part.at[3, chunk(n)], from_next.at[chunk(n)], dev_y(-1), "sum", "sum%d" % p).start()
            else:
                message(part.at[1, chunk(n)], from_prev.at[chunk(n)], dev_y(1), "sum", "sum%d" % p).start()

    def relay(n):
        at = chunk(n)
        waiting(relayed.at[at], "recv", "via%d" % n)
        mine = part[1 if n < 2 else 3, at, :]
        comb[at, :] = (mine.astype(F32) + relayed[at, :].astype(F32)).astype(BF16)
        got = "sum%d" % (n in (0, 3))
        if n < 2:
            message(comb.at[at], from_prev.at[at], dev_y(1), "sum", got).start()
        else:
            message(comb.at[at], from_next.at[at], dev_y(-1), "sum", got).start()

    with jax.named_scope("mix1"):
        mixers(1)
    with jax.named_scope("out_last_far"):
        outof.last_far()
    with jax.named_scope("mix2"):
        mixers(2)
    with jax.named_scope("out_order_near"):
        outof.in_order(wout_abs, NEAR, True)
    with jax.named_scope("out_order_far"):
        outof.in_order(wout_abs, FAR, True)
    with jax.named_scope("part12"):
        partials(0, 1, 2)
    with jax.named_scope("halo"):
        waiting(kv.at[pl.ds(0, 2 * WINDOW)], "recv", "kv")
        waiting(chan.at[pl.ds(0, 2 * RIM)], "recv", "ch")
    with jax.named_scope("mix03"):
        mixers(0, 3)
    with jax.named_scope("part03"):
        partials(1, 0, 3)
    with jax.named_scope("relay12"):
        relay(1)
        relay(2)
    with jax.named_scope("relay03"):
        relay(0)
        relay(3)

    lane = lax.broadcasted_iota(jnp.int32, (WINDOW, 128), 1)

    def settle(p, first, second):
        waiting(from_prev, "recv", "sum%d" % p)
        for k, n in enumerate((first, second)):
            at = chunk(n)
            mix = part[0, at, :].astype(F32) + from_prev[at, :].astype(F32) + from_next[at, :].astype(F32)
            share[at, :] = mix
            one = jnp.sum(mix, axis=1, keepdims=True)
            two = jnp.sum(mix * mix, axis=1, keepdims=True)
            both = jnp.where(lane == 0, one, jnp.where(lane == 1, two, 0.0))
            stats[4 * p, k * 8 : k * 8 + 8, :] = both.T[0:8]
        for d, slot in ((2, 2), (1, 3), (-1, 1)):
            message(stats.at[4 * p], stats.at[4 * p + slot], dev_y(d), "told%d" % p, "told%d" % p).start()

    width = feats * NY
    writes = []

    def finish(p, first, second):
        waiting(stats.at[pl.ds(0, 3)], "recv", "told%d" % p)
        for k, n in enumerate((first, second)):
            at = chunk(n)
            eight = slice(k * 8, k * 8 + 8)
            both = stats[4 * p, eight, :] + stats[4 * p + 1, eight, :]
            both = both + stats[4 * p + 2, eight, :] + stats[4 * p + 3, eight, :]
            both = jnp.concatenate([both] * 16, axis=0).T
            mean = both[:, 0:1] / width
            variance = both[:, 1:2] / width - mean * mean
            normed = (share[at, :] - mean) * lax.rsqrt(variance + epsilon) * gain[...]
            outv[at, :] = normed.astype(BF16)
            writes.append(pltpu.make_async_copy(outv.at[at], out_hbm.at[at], out_sem.at[n]))
            writes[-1].start()

    with jax.named_scope("settle12"):
        settle(0, 1, 2)
    with jax.named_scope("settle03"):
        settle(1, 0, 3)
    with jax.named_scope("finish12"):
        finish(0, 1, 2)
        into.sent()
        outof.sent()
        for ref, name in (
            (toks.at[pl.ds(0, 3)], "tok"), (part.at[pl.ds(0, 3)], "sum"), (kv.at[pl.ds(0, 2 * WINDOW)], "kv"),
            (chan.at[pl.ds(0, 2 * RIM)], "ch"), (stats.at[pl.ds(0, 3)], "told0"), (stats.at[pl.ds(0, 3)], "told1"),
        ):
            waiting(ref, "send", name)
    with jax.named_scope("finish03"):
        finish(1, 0, 3)
        for write in writes:
            write.wait()
    assert len(groups) == SEMAPHORES


SEMAPHORES = 57


def local(tokens, w_query, w_key, w_value, w_pool_in, sink, w_pool, pool_scale, w_out_attn, w_out_pool, out_gain):
    rows, feats = tokens.shape
    hbm = pl.BlockSpec(memory_space=pltpu.HBM)
    lanes_in = 640
    lanes_out = 512
    model = feats * NY
    return pl.pallas_call(
        kernel,
        out_shape=jax.ShapeDtypeStruct((rows, feats), BF16),
        in_specs=[hbm] * 11,
        out_specs=hbm,
        scratch_shapes=[
            pltpu.VMEM((NY, rows, feats), BF16),
            pltpu.VMEM((NX * NC * NZ, 16, lanes_in), BF16),
            pltpu.VMEM((NX * NC * NZ, 16, lanes_out), BF16),
            pltpu.VMEM((model, lanes_in), BF16),
            pltpu.VMEM((model, lanes_out), BF16),
            pltpu.VMEM((rows, 256), BF16),
            pltpu.VMEM((rows + 2 * WINDOW, 128), BF16),
            pltpu.VMEM((rows + 2 * RIM, 256), BF16),
            pltpu.VMEM((rows, lanes_out), BF16),
            pltpu.VMEM((NY, rows, feats), BF16),
            pltpu.VMEM((rows, feats), BF16),
            pltpu.VMEM((rows, feats), BF16),
            pltpu.VMEM((rows, feats), BF16),
            pltpu.VMEM((rows, feats), BF16),
            pltpu.VMEM((rows, feats), F32),
            pltpu.VMEM((2 * NY, 16, 128), F32),
            pltpu.VMEM((rows, model), BF16),
            pltpu.VMEM((rows, lanes_in), F32),
            pltpu.VMEM((16, 64), BF16),
            pltpu.VMEM((16, 64), BF16),
            pltpu.VMEM((1, 4), F32),
            pltpu.VMEM((1, 256, 256), BF16),
            pltpu.VMEM((1, 256), F32),
            pltpu.VMEM((1, 512), F32),
            pltpu.VMEM((rows, feats), BF16),
            pltpu.SemaphoreType.DMA((11,)),
            pltpu.SemaphoreType.DMA((4,)),
            pltpu.SemaphoreType.DMA((SEMAPHORES,)),
        ],
        compiler_params=pltpu.CompilerParams(
            collective_id=0, has_side_effects=True
        ),
    )(
        tokens, w_query, w_key, w_value, w_pool_in, sink.reshape(1, -1), w_pool, pool_scale.reshape(1, -1),
        w_out_attn.T, w_out_pool.T, out_gain.reshape(1, -1),
    )


def solution(mesh):
    finer = Mesh(mesh.devices.reshape(NZ, NX, NC, NY), (*SP, "tp"))
    return jax.shard_map(
        local,
        mesh=finer,
        in_specs=(
            P(SP, "tp"), P(SP, "tp"), P(SP, "tp"), P(SP, "tp"), P(SP, "tp"), P("tp"),
            P("tp", None, None), P("tp"), P("tp", SP), P("tp", SP), P("tp"),
        ),
        out_specs=P(SP, "tp"),
        check_vma=False,
    )
```

```python
import jax
import jax.numpy as jnp
from jax import lax
from jax.experimental import pallas as pl
from jax.experimental.pallas import tpu as pltpu
from jax.sharding import Mesh
from jax.sharding import PartitionSpec as P

HEAD_DIM = 64
WINDOW = 128
RIM = 16
SP = ("sp_0", "sp_1", "sp_2")
MESH = pl.DeviceIdType.MESH
NZ, NX, NC, NY = 16, 4, 2, 4

epsilon = 1e-05
masked_score = -1e30

OWN, NEAR, REST = 3, (0, 7), (7, 16)
FIRST, SECOND, MIDDLE, FAR = ((1, 4), (4, 6)), ((0, 1), (6, 7)), ((7, 10), (13, 16)), ((10, 12), (12, 13))
NT = (((1,), (1,)), ((), ()))
TN = (((0,), (0,)), ((), ()))
BF16, F32 = jnp.bfloat16, jnp.float32


def kernel(
    tok_hbm, wq_hbm, wk_hbm, wv_hbm, wc_hbm, sink_hbm, wpool_hbm, scale_hbm, woa_hbm, wop_hbm, gain_hbm,
    out_hbm,
    toks, win, wout, win_abs, wout_abs, query, kv, chan, hid, part, comb, relayed, from_prev, from_next,
    share, stats, turned_toks, acc, wk, wv, sink, wpool, scale, gain, outv, local_sem, out_sem, sems,
):
    z, x, c, y = (lax.axis_index(a) for a in (*SP, "tp"))
    rows, feats = toks.shape[1], toks.shape[2]
    seq_len = rows * NZ * NX * NC
    place = (z * NX + x) * NC + c
    offset = place * rows
    total_places = NZ * NX * NC

    def dev_z(d):
        return {"sp_0": lax.rem(z + (d + NZ), NZ)}

    def dev_x(d):
        return {"sp_1": lax.rem(x + (d + NX), NX)}

    def dev_y(d):
        return {"tp": lax.rem(y + (d + NY), NY)}

    dev_c = {"sp_2": 1 - c}

    def dev_sp(d):
        s = lax.rem(place + (d + total_places), total_places)
        return {
            "sp_0": lax.div(s, NX * NC),
            "sp_1": lax.rem(lax.div(s, NC), NX),
            "sp_2": lax.rem(s, NC),
        }

    peers = [dev_z(d) for d in (3, -3, 2, -2, 1, -1)]
    peers += [dev_y(2), dev_sp(1), dev_sp(-1), dev_x(1), dev_x(-1), dev_y(1), dev_y(-1), dev_c]
    mine_in, mine_out = win.at[OWN], wout.at[OWN]
    pairs = (
        (wk_hbm, wk), (wv_hbm, wv), (wq_hbm, mine_in.at[:, pl.ds(0, 256)]), (wc_hbm, mine_in.at[:, pl.ds(384, 256)]),
        (woa_hbm, mine_out.at[:, pl.ds(0, 256)]), (wop_hbm, mine_out.at[:, pl.ds(256, 256)]), (tok_hbm, toks.at[0]),
        (wpool_hbm, wpool), (scale_hbm, scale), (gain_hbm, gain), (sink_hbm, sink),
    )
    loads = [pltpu.make_async_copy(a, b, local_sem.at[k]) for k, (a, b) in enumerate(pairs)]
    for load in loads:
        load.start()

    barrier = pltpu.get_barrier_semaphore()
    for peer in peers:
        pl.semaphore_signal(barrier, inc=1, device_id=peer, device_id_type=MESH)

    with jax.named_scope("entry"):
        loads[0].wait()
        loads[1].wait()
        win[OWN, :, 256:384] = jnp.concatenate([wk[...], wv[...]], axis=1)
        for load in loads[2:6]:
            load.wait()
        pl.semaphore_wait(barrier, len(peers))

    groups = {}

    def message(src, dst, device, sent, got):
        for key in (("send", sent), ("recv", got)):
            groups.setdefault(key, len(groups))
        return pltpu.make_async_remote_copy(
            src_ref=src, dst_ref=dst, send_sem=sems.at[groups["send", sent]], recv_sem=sems.at[groups["recv", got]],
            device_id=device, device_id_type=MESH,
        )

    def waiting(ref, kind, name):
        sem = sems.at[groups[kind, name]]
        copy = pltpu.make_async_remote_copy(
            src_ref=ref, dst_ref=ref, send_sem=sem, recv_sem=sem, device_id=dev_c, device_id_type=MESH
        )
        if kind == "send":
            copy.wait_send()
        else:
            copy.wait_recv()

    class Gather:
        def __init__(self, w, name):
            self.w, self.name = w, name

        def at(self, r, k, lo, hi):
            return self.w.at[pl.ds((r * NC + k) * NZ + lo, hi - lo)]

        def send(self, src, dst, device, got):
            message(src, dst, device, self.name, self.name + got).start()

        def wait(self, slots, got):
            waiting(self.w.at[pl.ds(0, slots)], "recv", self.name + got)

        def pass_on(self, src, dst, d, got):
            self.send(self.at(0, 0, src, src + 1), self.at(0, 0, dst, dst + 1), dev_z(d), got)

        def near(self):
            for d in (1, -1, 2, -2, 3, -3):
                self.pass_on(OWN, (3 - d) % NZ, d, {3: "m3", -3: "p3"}.get(d, "n1"))

        def middle(self):
            self.wait(1, "m3")
            for e in (3, 2, 1):
                self.pass_on(0, 16 - e, e, "m6" if e == 3 else "mid")
            self.wait(1, "p3")
            for e in (3, 2, 1):
                self.pass_on(6, 6 + e, -e, "p6" if e == 3 else "mid")

        def far(self):
            self.wait(1, "m6")
            self.pass_on(13, 11, 2, "far")
            self.pass_on(13, 12, 1, "far")
            self.wait(1, "p6")
            self.pass_on(9, 10, -1, "far")

        def along_x(self, stage):
            up, down = stage
            others = "o%d" % (stage in (MIDDLE, FAR))
            self.send(self.at(0, 0, *up), self.at(3, 0, *up), dev_x(1), "x%d" % up[0])
            self.send(self.at(0, 0, *down), self.at(1, 0, *down), dev_x(-1), "x%d" % down[0])
            self.send(self.at(0, 0, *down), self.at(3, 0, *down), dev_x(1), others)
            self.send(self.at(0, 0, *up), self.at(1, 0, *up), dev_x(-1), others)

        def relay_x(self, stage):
            part = "rest" if stage in (MIDDLE, FAR) else "near"
            for r, d, span in ((3, 1, stage[0]), (1, -1, stage[1])):
                self.wait(span[1] - span[0], "x%d" % span[0])
                self.send(self.at(r, 0, *span), self.at(2, 0, *span), dev_x(d), "x2" + part)

        def across(self, r, span):
            part = "near" if span == NEAR else "rest"
            self.send(self.at(r, 0, *span), self.at(r, 1, *span), dev_c, "c" + part)

        def first(self):
            self.wait(4, "n1")
            self.along_x(FIRST)

        def second(self):
            self.along_x(SECOND)
            self.across(0, NEAR)

        def third(self):
            self.wait(4, "mid")
            self.along_x(MIDDLE)

        def fourth(self):
            self.wait(3, "far")
            self.along_x(FAR)
            self.across(0, REST)

        def others_near(self):
            self.wait(7, "o0")
            self.across(3, NEAR)
            self.across(1, NEAR)

        def others_rest(self):
            self.wait(9, "o1")
            self.across(3, REST)
            self.across(1, REST)

        def last_near(self):
            self.wait(7, "x2near")
            self.across(2, NEAR)

        def last_rest(self):
            self.wait(9, "x2rest")
            self.across(2, REST)

        def in_order(self, dest, span, turned):
            w = self.w
            self.wait(NX * (span[1] - span[0]), "cnear" if span == NEAR else "crest")

            def one(p, carry):
                base = (lax.rem(z + p + (NZ - OWN), NZ) if turned else p) * (NX * NC * 16)
                for r in range(NX):
                    for k in range(NC):
                        at = base + lax.rem(x + r, NX) * (NC * 16) + lax.rem(c + k, NC) * 16
                        dest[pl.ds(pl.multiple_of(at, 16), 16), :] = w[(r * NC + k) * NZ + p]
                return carry

            lax.fori_loop(*span, one, 0)

        def sent(self):
            waiting(self.w.at[pl.ds(0, 127)], "send", self.name)

    into = Gather(win, "in")
    outof = Gather(wout, "out")

    def chunk(b):
        return pl.ds(b * WINDOW, WINDOW)

    def tokens_to(slot, b, src, d, got):
        message(toks.at[src, chunk(b)], toks.at[slot, chunk(b)], dev_y(d), "tok", got).start()

    def tokens_relay(b):
        waiting(toks.at[0, chunk(0)], "recv", "tok%d" % b)
        if b < 2:
            tokens_to(2, b, 3, 1, "tok")
        else:
            tokens_to(2, b, 1, -1, "tok")

    with jax.named_scope("near"):
        into.near()
        loads[6].wait()
        for b in (0, 1):
            tokens_to(3, b, 0, 1, "tok%d" % b)
            tokens_to(1, b + 2, 0, -1, "tok%d" % (b + 2))
        for b in (0, 1):
            tokens_to(3, b + 2, 0, 1, "tok")
            tokens_to(1, b, 0, -1, "tok")
    with jax.named_scope("in_first"):
        into.first()
    with jax.named_scope("in_middle"):
        into.middle()
        outof.near()
        for load in loads[7:]:
            load.wait()
    with jax.named_scope("in_second"):
        into.second()
    with jax.named_scope("tok_relay_a"):
        tokens_relay(0)
        tokens_relay(2)
    with jax.named_scope("in_relay_first"):
        into.relay_x(FIRST)
    with jax.named_scope("in_far"):
        into.far()
    with jax.named_scope("in_third"):
        into.third()
    with jax.named_scope("tok_relay_b"):
        tokens_relay(1)
        tokens_relay(3)
    with jax.named_scope("in_relay_second"):
        into.relay_x(SECOND)
    with jax.named_scope("out_middle"):
        outof.middle()
    with jax.named_scope("in_others_near"):
        into.others_near()
    with jax.named_scope("in_fourth"):
        into.fourth()
    with jax.named_scope("in_relay_third"):
        into.relay_x(MIDDLE)
    with jax.named_scope("out_first"):
        outof.first()
    with jax.named_scope("in_last_near"):
        into.last_near()
    with jax.named_scope("out_far"):
        outof.far()
    with jax.named_scope("in_relay_fourth"):
        into.relay_x(FAR)
    with jax.named_scope("out_second"):
        outof.second()
    with jax.named_scope("in_others_rest"):
        into.others_rest()
    with jax.named_scope("out_third"):
        outof.third()
    with jax.named_scope("in_order_near"):
        into.in_order(win_abs, NEAR, False)
    with jax.named_scope("out_fourth"):
        outof.fourth()
    with jax.named_scope("tok_done"):
        waiting(toks.at[pl.ds(0, 2)], "recv", "tok")
        for p in range(NZ):
            at = lax.rem(z + (p + NZ - OWN), NZ)
            per = feats // 128
            r = lax.rem(lax.div(at, per) + (NY - y), NY)
            cols = pl.ds(pl.multiple_of(lax.rem(at, per) * 128, 128), 128)
            turned_toks[:, p * 128 : (p + 1) * 128] = toks[r, :, cols]

    with jax.named_scope("out_relay_first"):
        outof.relay_x(FIRST)
    with jax.named_scope("in_last_rest"):
        into.last_rest()
    with jax.named_scope("out_relay_second"):
        outof.relay_x(SECOND)
    with jax.named_scope("out_relay_third"):
        outof.relay_x(MIDDLE)
        outof.others_near()
    parts = ((256, 384), (384, 640), (0, 256))
    with jax.named_scope("project_near"):
        depth = slice(NEAR[0] * 128, NEAR[1] * 128)
        for lo, hi in parts:
            acc[:, lo:hi] = jnp.dot(turned_toks[:, depth], win_abs[depth, lo:hi], preferred_element_type=F32)
    with jax.named_scope("in_order_rest"):
        into.in_order(win_abs, REST, False)

    with jax.named_scope("out_relay_fourth"):
        outof.relay_x(FAR)
        outof.others_rest()

    def project(lo, hi):
        depth = slice(REST[0] * 128, REST[1] * 128)
        return acc[:, lo:hi] + jnp.dot(turned_toks[:, depth], win_abs[depth, lo:hi], preferred_element_type=F32)

    own_kv, own_ch = (kv, WINDOW, "kv"), (chan, RIM, "ch")

    def to_neighbours(ref, size, name):
        message(ref.at[pl.ds(rows, size)], ref.at[pl.ds(0, size)], dev_sp(1), name, name).start()
        message(ref.at[pl.ds(size, size)], ref.at[pl.ds(size + rows, size)], dev_sp(-1), name, name).start()

    with jax.named_scope("project"):
        kv[pl.ds(WINDOW, rows), :] = project(256, 384).astype(BF16)
        chan[pl.ds(RIM, rows), :] = project(384, 640).astype(BF16)
        query[...] = (project(0, 256) * HEAD_DIM ** (-0.5)).astype(BF16)
        to_neighbours(*own_kv)
        to_neighbours(*own_ch)

    with jax.named_scope("out_last_near"):
        outof.last_near()

    half = lax.shift_left(jnp.int32(1), y.astype(jnp.int32))
    sinks = jnp.concatenate([jnp.broadcast_to(sink[0:1, h : h + 1], (1, WINDOW)) for h in range(4)], axis=1)

    def attend(n):
        first = offset + n * WINDOW
        band = kv[pl.ds(n * WINDOW, 3 * WINDOW), :]
        keys, values = band[:, :HEAD_DIM], band[:, HEAD_DIM:]
        block = query[n * WINDOW : (n + 1) * WINDOW, :]
        stacked = jnp.concatenate([block[:, h * HEAD_DIM : (h + 1) * HEAD_DIM] for h in range(4)], axis=0)
        scores = lax.dot_general(keys, stacked, NT, preferred_element_type=F32)
        j = lax.broadcasted_iota(jnp.int32, (WINDOW, 4 * WINDOW), 0)
        i = lax.rem(lax.broadcasted_iota(jnp.int32, (WINDOW, 4 * WINDOW), 1), WINDOW)
        before = jnp.where((j >= i) & (first > 0), scores[:WINDOW], masked_score)
        here = scores[WINDOW : 2 * WINDOW]
        after = jnp.where((j <= i) & (first + WINDOW < seq_len), scores[2 * WINDOW :], masked_score)
        top = jnp.max(jnp.maximum(jnp.maximum(before, here), after), axis=0, keepdims=True)
        top = jnp.maximum(top, sinks)
        before, here, after = jnp.exp(before - top), jnp.exp(here - top), jnp.exp(after - top)
        total = jnp.sum(before + here + after, axis=0, keepdims=True) + jnp.exp(sinks - top)
        inverse = 1.0 / total
        probs = jnp.concatenate([(r * inverse).astype(BF16) for r in (before, here, after)], axis=0)
        out = lax.dot_general(values, probs, TN, preferred_element_type=F32)
        out = jnp.concatenate([out[:, h * WINDOW : (h + 1) * WINDOW] for h in range(4)], axis=0)
        hid[n * WINDOW : (n + 1) * WINDOW, 0:256] = out.T.astype(BF16)

    def pool(n):
        first = offset + n * WINDOW
        i = lax.broadcasted_iota(jnp.int32, (WINDOW, WINDOW + 2 * RIM), 0)
        j = lax.broadcasted_iota(jnp.int32, (WINDOW, WINDOW + 2 * RIM), 1) - RIM
        pos = first + j
        member = (j >= i - half) & (j < i + half) & (pos >= 0) & (pos < seq_len)
        member = jnp.where(member, 1.0, 0.0).astype(BF16)
        sums = jnp.dot(member, chan[pl.ds(n * WINDOW, WINDOW + 2 * RIM), :], preferred_element_type=F32)
        t = first + lax.broadcasted_iota(jnp.int32, (WINDOW, 1), 0)
        count = (jnp.minimum(t + half, seq_len) - jnp.maximum(t - half, 0)).astype(F32)
        spread = (sums / count - chan[pl.ds(n * WINDOW + RIM, WINDOW), :].astype(F32)).astype(BF16)
        pooled = jnp.dot(spread, wpool[0], preferred_element_type=F32) * scale[...]
        hid[n * WINDOW : (n + 1) * WINDOW, 256:512] = pooled.astype(BF16)

    def mixers(*which):
        for n in which:
            pool(n)
            attend(n)

    def partials(p, first, second):
        both = jnp.concatenate([hid[chunk(first), :], hid[chunk(second), :]], axis=0)
        for d in (2, 3, 1, 0):
            cols = pl.ds(pl.multiple_of(lax.rem(y + d, NY) * feats, feats), feats)
            terms = lax.dot_general(both, wout_abs[cols, :], NT, preferred_element_type=F32).astype(BF16)
            part[d, chunk(first), :] = terms[:WINDOW]
            part[d, chunk(second), :] = terms[WINDOW:]
        for n in (first, second):
            target = dev_y(1 if n < 2 else -1)
            message(part.at[2, chunk(n)], relayed.at[chunk(n)], target, "sum", "via%d" % n).start()
        for n in (first, second):
            if n < 2:
                message(part.at[3, chunk(n)], from_next.at[chunk(n)], dev_y(-1), "sum", "sum%d" % p).start()
            else:
                message(part.at[1, chunk(n)], from_prev.at[chunk(n)], dev_y(1), "sum", "sum%d" % p).start()

    def relay(n):
        at = chunk(n)
        waiting(relayed.at[at], "recv", "via%d" % n)
        mine = part[1 if n < 2 else 3, at, :]
        comb[at, :] = (mine.astype(F32) + relayed[at, :].astype(F32)).astype(BF16)
        got = "sum%d" % (n in (0, 3))
        if n < 2:
            message(comb.at[at], from_prev.at[at], dev_y(1), "sum", got).start()
        else:
            message(comb.at[at], from_next.at[at], dev_y(-1), "sum", got).start()

    with jax.named_scope("mix1"):
        mixers(1)
    with jax.named_scope("out_last_rest"):
        outof.last_rest()
    with jax.named_scope("mix2"):
        mixers(2)
    with jax.named_scope("out_order_near"):
        outof.in_order(wout_abs, NEAR, True)
    with jax.named_scope("out_order_rest"):
        outof.in_order(wout_abs, REST, True)
    with jax.named_scope("part12"):
        partials(0, 1, 2)
    with jax.named_scope("halo"):
        waiting(kv.at[pl.ds(0, 2 * WINDOW)], "recv", "kv")
        waiting(chan.at[pl.ds(0, 2 * RIM)], "recv", "ch")
    with jax.named_scope("mix03"):
        mixers(0, 3)
    with jax.named_scope("part03"):
        partials(1, 0, 3)
    with jax.named_scope("relay12"):
        relay(1)
        relay(2)
    with jax.named_scope("relay03"):
        relay(0)
        relay(3)

    lane = lax.broadcasted_iota(jnp.int32, (WINDOW, 128), 1)

    def settle(p, first, second):
        waiting(from_prev, "recv", "sum%d" % p)
        for k, n in enumerate((first, second)):
            at = chunk(n)
            mix = part[0, at, :].astype(F32) + from_prev[at, :].astype(F32) + from_next[at, :].astype(F32)
            share[at, :] = mix
            one = jnp.sum(mix, axis=1, keepdims=True)
            two = jnp.sum(mix * mix, axis=1, keepdims=True)
            both = jnp.where(lane == 0, one, jnp.where(lane == 1, two, 0.0))
            stats[4 * p, k * 8 : k * 8 + 8, :] = both.T[0:8]
        for d, slot in ((2, 2), (1, 3), (-1, 1)):
            message(stats.at[4 * p], stats.at[4 * p + slot], dev_y(d), "told%d" % p, "told%d" % p).start()

    width = feats * NY
    writes = []

    def finish(p, first, second):
        waiting(stats.at[pl.ds(0, 3)], "recv", "told%d" % p)
        for k, n in enumerate((first, second)):
            at = chunk(n)
            eight = slice(k * 8, k * 8 + 8)
            both = stats[4 * p, eight, :] + stats[4 * p + 1, eight, :]
            both = both + stats[4 * p + 2, eight, :] + stats[4 * p + 3, eight, :]
            both = jnp.concatenate([both] * 16, axis=0).T
            mean = both[:, 0:1] / width
            variance = both[:, 1:2] / width - mean * mean
            normed = (share[at, :] - mean) * lax.rsqrt(variance + epsilon) * gain[...]
            outv[at, :] = normed.astype(BF16)
            writes.append(pltpu.make_async_copy(outv.at[at], out_hbm.at[at], out_sem.at[n]))
            writes[-1].start()

    with jax.named_scope("settle12"):
        settle(0, 1, 2)
    with jax.named_scope("settle03"):
        settle(1, 0, 3)
    with jax.named_scope("finish12"):
        finish(0, 1, 2)
        into.sent()
        outof.sent()
        for ref, name in (
            (toks.at[pl.ds(0, 3)], "tok"), (part.at[pl.ds(0, 3)], "sum"), (kv.at[pl.ds(0, 2 * WINDOW)], "kv"),
            (chan.at[pl.ds(0, 2 * RIM)], "ch"), (stats.at[pl.ds(0, 3)], "told0"), (stats.at[pl.ds(0, 3)], "told1"),
        ):
            waiting(ref, "send", name)
    with jax.named_scope("finish03"):
        finish(1, 0, 3)
        for write in writes:
            write.wait()
    assert len(groups) == SEMAPHORES


SEMAPHORES = 65


def local(tokens, w_query, w_key, w_value, w_pool_in, sink, w_pool, pool_scale, w_out_attn, w_out_pool, out_gain):
    rows, feats = tokens.shape
    hbm = pl.BlockSpec(memory_space=pltpu.HBM)
    lanes_in = 640
    lanes_out = 512
    model = feats * NY
    return pl.pallas_call(
        kernel,
        out_shape=jax.ShapeDtypeStruct((rows, feats), BF16),
        in_specs=[hbm] * 11,
        out_specs=hbm,
        scratch_shapes=[
            pltpu.VMEM((NY, rows, feats), BF16),
            pltpu.VMEM((NX * NC * NZ, 16, lanes_in), BF16),
            pltpu.VMEM((NX * NC * NZ, 16, lanes_out), BF16),
            pltpu.VMEM((model, lanes_in), BF16),
            pltpu.VMEM((model, lanes_out), BF16),
            pltpu.VMEM((rows, 256), BF16),
            pltpu.VMEM((rows + 2 * WINDOW, 128), BF16),
            pltpu.VMEM((rows + 2 * RIM, 256), BF16),
            pltpu.VMEM((rows, lanes_out), BF16),
            pltpu.VMEM((NY, rows, feats), BF16),
            pltpu.VMEM((rows, feats), BF16),
            pltpu.VMEM((rows, feats), BF16),
            pltpu.VMEM((rows, feats), BF16),
            pltpu.VMEM((rows, feats), BF16),
            pltpu.VMEM((rows, feats), F32),
            pltpu.VMEM((2 * NY, 16, 128), F32),
            pltpu.VMEM((rows, model), BF16),
            pltpu.VMEM((rows, lanes_in), F32),
            pltpu.VMEM((16, 64), BF16),
            pltpu.VMEM((16, 64), BF16),
            pltpu.VMEM((1, 4), F32),
            pltpu.VMEM((1, 256, 256), BF16),
            pltpu.VMEM((1, 256), F32),
            pltpu.VMEM((1, 512), F32),
            pltpu.VMEM((rows, feats), BF16),
            pltpu.SemaphoreType.DMA((11,)),
            pltpu.SemaphoreType.DMA((4,)),
            pltpu.SemaphoreType.DMA((SEMAPHORES,)),
        ],
        compiler_params=pltpu.CompilerParams(
            collective_id=0, has_side_effects=True
        ),
    )(
        tokens, w_query, w_key, w_value, w_pool_in, sink.reshape(1, -1), w_pool, pool_scale.reshape(1, -1),
        w_out_attn.T, w_out_pool.T, out_gain.reshape(1, -1),
    )


def solution(mesh):
    finer = Mesh(mesh.devices.reshape(NZ, NX, NC, NY), (*SP, "tp"))
    return jax.shard_map(
        local,
        mesh=finer,
        in_specs=(
            P(SP, "tp"), P(SP, "tp"), P(SP, "tp"), P(SP, "tp"), P(SP, "tp"), P("tp"),
            P("tp", None, None), P("tp"), P("tp", SP), P("tp", SP), P("tp"),
        ),
        out_specs=P(SP, "tp"),
        check_vma=False,
    )
```

```python
import jax
import jax.numpy as jnp
from jax import lax
from jax.experimental import pallas as pl
from jax.experimental.pallas import tpu as pltpu
from jax.sharding import Mesh
from jax.sharding import PartitionSpec as P

HEAD_DIM = 64
WINDOW = 128
RIM = 16
SP = ("sp_0", "sp_1", "sp_2")
MESH = pl.DeviceIdType.MESH
NZ, NX, NC, NY = 16, 4, 2, 4

epsilon = 1e-05
masked_score = -1e30

OWN, NEAR, REST = 3, (0, 7), (7, 16)
FIRST, SECOND, MIDDLE, FAR = ((1, 4), (4, 6)), ((0, 1), (6, 7)), ((7, 10), (13, 16)), ((10, 12), (12, 13))
NT = (((1,), (1,)), ((), ()))
TN = (((0,), (0,)), ((), ()))
BF16, F32 = jnp.bfloat16, jnp.float32


def kernel(
    tok_hbm, wq_hbm, wk_hbm, wv_hbm, wc_hbm, sink_hbm, wpool_hbm, scale_hbm, woa_hbm, wop_hbm, gain_hbm,
    out_hbm,
    toks, win, wout, win_abs, wout_abs, query, kv, chan, hid, part, comb, relayed, from_prev, from_next,
    share, stats, turned_toks, acc, wk, wv, sink, wpool, scale, gain, outv, local_sem, out_sem, sems,
):
    z, x, c, y = (lax.axis_index(a) for a in (*SP, "tp"))
    rows, feats = toks.shape[1], toks.shape[2]
    seq_len = rows * NZ * NX * NC
    place = (z * NX + x) * NC + c
    offset = place * rows
    total_places = NZ * NX * NC

    def dev_z(d):
        return {"sp_0": lax.rem(z + (d + NZ), NZ)}

    def dev_x(d):
        return {"sp_1": lax.rem(x + (d + NX), NX)}

    def dev_y(d):
        return {"tp": lax.rem(y + (d + NY), NY)}

    dev_c = {"sp_2": 1 - c}

    def dev_sp(d):
        s = lax.rem(place + (d + total_places), total_places)
        return {
            "sp_0": lax.div(s, NX * NC),
            "sp_1": lax.rem(lax.div(s, NC), NX),
            "sp_2": lax.rem(s, NC),
        }

    peers = [dev_z(d) for d in (3, -3, 2, -2, 1, -1)]
    peers += [dev_y(2), dev_sp(1), dev_sp(-1), dev_x(1), dev_x(-1), dev_y(1), dev_y(-1), dev_c]
    mine_in, mine_out = win.at[OWN], wout.at[OWN]
    pairs = (
        (wk_hbm, wk), (wv_hbm, wv), (wq_hbm, mine_in.at[:, pl.ds(0, 256)]), (wc_hbm, mine_in.at[:, pl.ds(384, 256)]),
        (woa_hbm, mine_out.at[:, pl.ds(0, 256)]), (wop_hbm, mine_out.at[:, pl.ds(256, 256)]), (tok_hbm, toks.at[0]),
        (wpool_hbm, wpool), (scale_hbm, scale), (gain_hbm, gain), (sink_hbm, sink),
    )
    loads = [pltpu.make_async_copy(a, b, local_sem.at[k]) for k, (a, b) in enumerate(pairs)]
    for load in loads:
        load.start()

    barrier = pltpu.get_barrier_semaphore()
    for peer in peers:
        pl.semaphore_signal(barrier, inc=1, device_id=peer, device_id_type=MESH)

    with jax.named_scope("entry"):
        loads[0].wait()
        loads[1].wait()
        win[OWN, :, 256:384] = jnp.concatenate([wk[...], wv[...]], axis=1)
        for load in loads[2:6]:
            load.wait()
        pl.semaphore_wait(barrier, len(peers))

    groups = {}

    def message(src, dst, device, sent, got):
        for key in (("send", sent), ("recv", got)):
            groups.setdefault(key, len(groups))
        return pltpu.make_async_remote_copy(
            src_ref=src, dst_ref=dst, send_sem=sems.at[groups["send", sent]], recv_sem=sems.at[groups["recv", got]],
            device_id=device, device_id_type=MESH,
        )

    def waiting(ref, kind, name):
        sem = sems.at[groups[kind, name]]
        copy = pltpu.make_async_remote_copy(
            src_ref=ref, dst_ref=ref, send_sem=sem, recv_sem=sem, device_id=dev_c, device_id_type=MESH
        )
        if kind == "send":
            copy.wait_send()
        else:
            copy.wait_recv()

    class Gather:
        def __init__(self, w, name):
            self.w, self.name = w, name

        def at(self, r, k, lo, hi):
            return self.w.at[pl.ds((r * NC + k) * NZ + lo, hi - lo)]

        def send(self, src, dst, device, got):
            message(src, dst, device, self.name, self.name + got).start()

        def wait(self, slots, got):
            waiting(self.w.at[pl.ds(0, slots)], "recv", self.name + got)

        def pass_on(self, src, dst, d, got):
            self.send(self.at(0, 0, src, src + 1), self.at(0, 0, dst, dst + 1), dev_z(d), got)

        def near(self):
            for d in (1, -1, 2, -2, 3, -3):
                self.pass_on(OWN, (3 - d) % NZ, d, {3: "m3", -3: "p3"}.get(d, "n1"))

        def middle(self):
            self.wait(1, "m3")
            for e in (3, 2, 1):
                self.pass_on(0, 16 - e, e, "m6" if e == 3 else "mid")
            self.wait(1, "p3")
            for e in (3, 2, 1):
                self.pass_on(6, 6 + e, -e, "p6" if e == 3 else "mid")

        def far(self):
            self.wait(1, "m6")
            self.pass_on(13, 11, 2, "far")
            self.pass_on(13, 12, 1, "far")
            self.wait(1, "p6")
            self.pass_on(9, 10, -1, "far")

        def along_x(self, stage):
            up, down = stage
            others = "o%d" % (stage in (MIDDLE, FAR))
            self.send(self.at(0, 0, *up), self.at(3, 0, *up), dev_x(1), "x%d" % up[0])
            self.send(self.at(0, 0, *down), self.at(1, 0, *down), dev_x(-1), "x%d" % down[0])
            self.send(self.at(0, 0, *down), self.at(3, 0, *down), dev_x(1), others)
            self.send(self.at(0, 0, *up), self.at(1, 0, *up), dev_x(-1), others)

        def relay_x(self, stage):
            part = "rest" if stage in (MIDDLE, FAR) else "near"
            for r, d, span in ((3, 1, stage[0]), (1, -1, stage[1])):
                self.wait(span[1] - span[0], "x%d" % span[0])
                self.send(self.at(r, 0, *span), self.at(2, 0, *span), dev_x(d), "x2" + part)

        def across(self, r, span):
            part = "near" if span == NEAR else "rest"
            self.send(self.at(r, 0, *span), self.at(r, 1, *span), dev_c, "c" + part)

        def first(self):
            self.wait(4, "n1")
            self.along_x(FIRST)

        def second(self):
            self.along_x(SECOND)
            self.across(0, NEAR)

        def third(self):
            self.wait(4, "mid")
            self.along_x(MIDDLE)

        def fourth(self):
            self.wait(3, "far")
            self.along_x(FAR)
            self.across(0, REST)

        def others_near(self):
            self.wait(7, "o0")
            self.across(3, NEAR)
            self.across(1, NEAR)

        def others_rest(self):
            self.wait(9, "o1")
            self.across(3, REST)
            self.across(1, REST)

        def last_near(self):
            self.wait(7, "x2near")
            self.across(2, NEAR)

        def last_rest(self):
            self.wait(9, "x2rest")
            self.across(2, REST)

        def in_order(self, dest, span, turned):
            w = self.w
            self.wait(NX * (span[1] - span[0]), "cnear" if span == NEAR else "crest")

            def one(p, carry):
                base = (lax.rem(z + p + (NZ - OWN), NZ) if turned else p) * (NX * NC * 16)
                for r in range(NX):
                    for k in range(NC):
                        at = base + lax.rem(x + r, NX) * (NC * 16) + lax.rem(c + k, NC) * 16
                        dest[pl.ds(pl.multiple_of(at, 16), 16), :] = w[(r * NC + k) * NZ + p]
                return carry

            lax.fori_loop(*span, one, 0)

        def sent(self):
            waiting(self.w.at[pl.ds(0, 127)], "send", self.name)

    into = Gather(win, "in")
    outof = Gather(wout, "out")

    def chunk(b):
        return pl.ds(b * WINDOW, WINDOW)

    def tokens_to(slot, b, src, d, got):
        message(toks.at[src, chunk(b)], toks.at[slot, chunk(b)], dev_y(d), "tok", got).start()

    def tokens_relay(b):
        waiting(toks.at[0, chunk(0)], "recv", "tok%d" % b)
        if b < 2:
            tokens_to(2, b, 3, 1, "tok")
        else:
            tokens_to(2, b, 1, -1, "tok")

    with jax.named_scope("near"):
        into.near()
        loads[6].wait()
        for b in (0, 1):
            tokens_to(3, b, 0, 1, "tok%d" % b)
            tokens_to(1, b + 2, 0, -1, "tok%d" % (b + 2))
        for b in (0, 1):
            tokens_to(3, b + 2, 0, 1, "tok")
            tokens_to(1, b, 0, -1, "tok")
    with jax.named_scope("in_first"):
        into.first()
    with jax.named_scope("in_middle"):
        into.middle()
        outof.near()
        for load in loads[7:]:
            load.wait()
    with jax.named_scope("in_second"):
        into.second()
    with jax.named_scope("tok_relay_a"):
        tokens_relay(0)
        tokens_relay(2)
    with jax.named_scope("in_relay_first"):
        into.relay_x(FIRST)
    with jax.named_scope("in_far"):
        into.far()
    with jax.named_scope("in_third"):
        into.third()
    with jax.named_scope("tok_relay_b"):
        tokens_relay(1)
        tokens_relay(3)
    with jax.named_scope("in_relay_second"):
        into.relay_x(SECOND)
    with jax.named_scope("out_middle"):
        outof.middle()
    with jax.named_scope("in_others_near"):
        into.others_near()
    with jax.named_scope("in_fourth"):
        into.fourth()
    with jax.named_scope("in_relay_third"):
        into.relay_x(MIDDLE)
    with jax.named_scope("out_first"):
        outof.first()
    with jax.named_scope("in_last_near"):
        into.last_near()
    with jax.named_scope("out_far"):
        outof.far()
    with jax.named_scope("in_relay_fourth"):
        into.relay_x(FAR)
    with jax.named_scope("out_second"):
        outof.second()
    with jax.named_scope("in_others_rest"):
        into.others_rest()
    with jax.named_scope("out_third"):
        outof.third()
    with jax.named_scope("in_order_near"):
        into.in_order(win_abs, NEAR, False)
    with jax.named_scope("out_fourth"):
        outof.fourth()
    with jax.named_scope("tok_done"):
        waiting(toks.at[pl.ds(0, 2)], "recv", "tok")
        for p in range(NZ):
            at = lax.rem(z + (p + NZ - OWN), NZ)
            per = feats // 128
            r = lax.rem(lax.div(at, per) + (NY - y), NY)
            cols = pl.ds(pl.multiple_of(lax.rem(at, per) * 128, 128), 128)
            turned_toks[:, p * 128 : (p + 1) * 128] = toks[r, :, cols]

    with jax.named_scope("out_relay_first"):
        outof.relay_x(FIRST)
    with jax.named_scope("in_last_rest"):
        into.last_rest()
    with jax.named_scope("out_relay_second"):
        outof.relay_x(SECOND)
    parts = ((256, 384), (384, 640), (0, 256))
    with jax.named_scope("project_near"):
        depth = slice(NEAR[0] * 128, NEAR[1] * 128)
        for lo, hi in parts:
            acc[:, lo:hi] = jnp.dot(turned_toks[:, depth], win_abs[depth, lo:hi], preferred_element_type=F32)
    with jax.named_scope("out_relay_third"):
        outof.relay_x(MIDDLE)
        outof.others_near()
    with jax.named_scope("in_order_rest"):
        into.in_order(win_abs, REST, False)

    with jax.named_scope("out_relay_fourth"):
        outof.relay_x(FAR)
        outof.others_rest()

    def project(lo, hi):
        depth = slice(REST[0] * 128, REST[1] * 128)
        return acc[:, lo:hi] + jnp.dot(turned_toks[:, depth], win_abs[depth, lo:hi], preferred_element_type=F32)

    own_kv, own_ch = (kv, WINDOW, "kv"), (chan, RIM, "ch")

    def to_neighbours(ref, size, name):
        message(ref.at[pl.ds(rows, size)], ref.at[pl.ds(0, size)], dev_sp(1), name, name).start()
        message(ref.at[pl.ds(size, size)], ref.at[pl.ds(size + rows, size)], dev_sp(-1), name, name).start()

    with jax.named_scope("project"):
        kv[pl.ds(WINDOW, rows), :] = project(256, 384).astype(BF16)
        chan[pl.ds(RIM, rows), :] = project(384, 640).astype(BF16)
        query[...] = (project(0, 256) * HEAD_DIM ** (-0.5)).astype(BF16)
        to_neighbours(*own_kv)
        to_neighbours(*own_ch)

    with jax.named_scope("out_last_near"):
        outof.last_near()

    half = lax.shift_left(jnp.int32(1), y.astype(jnp.int32))
    sinks = jnp.concatenate([jnp.broadcast_to(sink[0:1, h : h + 1], (1, WINDOW)) for h in range(4)], axis=1)

    def attend(n):
        first = offset + n * WINDOW
        band = kv[pl.ds(n * WINDOW, 3 * WINDOW), :]
        keys, values = band[:, :HEAD_DIM], band[:, HEAD_DIM:]
        block = query[n * WINDOW : (n + 1) * WINDOW, :]
        stacked = jnp.concatenate([block[:, h * HEAD_DIM : (h + 1) * HEAD_DIM] for h in range(4)], axis=0)
        scores = lax.dot_general(keys, stacked, NT, preferred_element_type=F32)
        j = lax.broadcasted_iota(jnp.int32, (WINDOW, 4 * WINDOW), 0)
        i = lax.rem(lax.broadcasted_iota(jnp.int32, (WINDOW, 4 * WINDOW), 1), WINDOW)
        before = jnp.where((j >= i) & (first > 0), scores[:WINDOW], masked_score)
        here = scores[WINDOW : 2 * WINDOW]
        after = jnp.where((j <= i) & (first + WINDOW < seq_len), scores[2 * WINDOW :], masked_score)
        top = jnp.max(jnp.maximum(jnp.maximum(before, here), after), axis=0, keepdims=True)
        top = jnp.maximum(top, sinks)
        before, here, after = jnp.exp(before - top), jnp.exp(here - top), jnp.exp(after - top)
        total = jnp.sum(before + here + after, axis=0, keepdims=True) + jnp.exp(sinks - top)
        inverse = 1.0 / total
        probs = jnp.concatenate([(r * inverse).astype(BF16) for r in (before, here, after)], axis=0)
        out = lax.dot_general(values, probs, TN, preferred_element_type=F32)
        out = jnp.concatenate([out[:, h * WINDOW : (h + 1) * WINDOW] for h in range(4)], axis=0)
        hid[n * WINDOW : (n + 1) * WINDOW, 0:256] = out.T.astype(BF16)

    def pool(n):
        first = offset + n * WINDOW
        i = lax.broadcasted_iota(jnp.int32, (WINDOW, WINDOW + 2 * RIM), 0)
        j = lax.broadcasted_iota(jnp.int32, (WINDOW, WINDOW + 2 * RIM), 1) - RIM
        pos = first + j
        member = (j >= i - half) & (j < i + half) & (pos >= 0) & (pos < seq_len)
        member = jnp.where(member, 1.0, 0.0).astype(BF16)
        sums = jnp.dot(member, chan[pl.ds(n * WINDOW, WINDOW + 2 * RIM), :], preferred_element_type=F32)
        t = first + lax.broadcasted_iota(jnp.int32, (WINDOW, 1), 0)
        count = (jnp.minimum(t + half, seq_len) - jnp.maximum(t - half, 0)).astype(F32)
        spread = (sums / count - chan[pl.ds(n * WINDOW + RIM, WINDOW), :].astype(F32)).astype(BF16)
        pooled = jnp.dot(spread, wpool[0], preferred_element_type=F32) * scale[...]
        hid[n * WINDOW : (n + 1) * WINDOW, 256:512] = pooled.astype(BF16)

    def mixers(*which):
        for n in which:
            pool(n)
            attend(n)

    def partials(p, first, second):
        both = jnp.concatenate([hid[chunk(first), :], hid[chunk(second), :]], axis=0)

        def terms(d):
            cols = pl.ds(pl.multiple_of(lax.rem(y + d, NY) * feats, feats), feats)
            out = lax.dot_general(both, wout_abs[cols, :], NT, preferred_element_type=F32).astype(BF16)
            part[d, chunk(first), :] = out[:WINDOW]
            part[d, chunk(second), :] = out[WINDOW:]

        terms(2)
        for n in (first, second):
            target = dev_y(1 if n < 2 else -1)
            message(part.at[2, chunk(n)], relayed.at[chunk(n)], target, "sum", "via%d" % n).start()
        for d in (3, 1, 0):
            terms(d)
        for n in (first, second):
            if n < 2:
                message(part.at[3, chunk(n)], from_next.at[chunk(n)], dev_y(-1), "sum", "one%d" % p).start()
            else:
                message(part.at[1, chunk(n)], from_prev.at[chunk(n)], dev_y(1), "sum", "one%d" % p).start()

    def relay(n):
        at = chunk(n)
        waiting(relayed.at[at], "recv", "via%d" % n)
        mine = part[1 if n < 2 else 3, at, :]
        comb[at, :] = (mine.astype(F32) + relayed[at, :].astype(F32)).astype(BF16)
        got = "sum%d" % (n in (0, 3))
        if n < 2:
            message(comb.at[at], from_prev.at[at], dev_y(1), "sum", got).start()
        else:
            message(comb.at[at], from_next.at[at], dev_y(-1), "sum", got).start()

    with jax.named_scope("mix1"):
        mixers(1)
    with jax.named_scope("out_last_rest"):
        outof.last_rest()
    with jax.named_scope("mix2"):
        mixers(2)
    with jax.named_scope("out_order_near"):
        outof.in_order(wout_abs, NEAR, True)
    with jax.named_scope("out_order_rest"):
        outof.in_order(wout_abs, REST, True)
    with jax.named_scope("part12"):
        partials(0, 1, 2)
    with jax.named_scope("halo"):
        waiting(kv.at[pl.ds(0, 2 * WINDOW)], "recv", "kv")
        waiting(chan.at[pl.ds(0, 2 * RIM)], "recv", "ch")
    with jax.named_scope("mix03"):
        mixers(0, 3)
    with jax.named_scope("part03"):
        partials(1, 0, 3)
    lane = lax.broadcasted_iota(jnp.int32, (WINDOW, 128), 1)

    def prepare(p, first, second):
        waiting(from_prev.at[pl.ds(0, 2 * WINDOW)], "recv", "one%d" % p)
        for n in (first, second):
            at = chunk(n)
            single = (from_next if n < 2 else from_prev)[at, :]
            share[at, :] = part[0, at, :].astype(F32) + single.astype(F32)

    def settle(p, first, second):
        waiting(from_prev.at[pl.ds(0, 2 * WINDOW)], "recv", "sum%d" % p)
        for k, n in enumerate((first, second)):
            at = chunk(n)
            mix = share[at, :] + (from_prev if n < 2 else from_next)[at, :].astype(F32)
            share[at, :] = mix
            one = jnp.sum(mix, axis=1, keepdims=True)
            two = jnp.sum(mix * mix, axis=1, keepdims=True)
            both = jnp.where(lane == 0, one, jnp.where(lane == 1, two, 0.0))
            stats[4 * p, k * 8 : k * 8 + 8, :] = both.T[0:8]
        for d, slot in ((2, 2), (1, 3), (-1, 1)):
            message(stats.at[4 * p], stats.at[4 * p + slot], dev_y(d), "told%d" % p, "told%d" % p).start()

    width = feats * NY
    writes = []

    def finish(p, first, second):
        waiting(stats.at[pl.ds(0, 3)], "recv", "told%d" % p)
        for k, n in enumerate((first, second)):
            at = chunk(n)
            eight = slice(k * 8, k * 8 + 8)
            both = stats[4 * p, eight, :] + stats[4 * p + 1, eight, :]
            both = both + stats[4 * p + 2, eight, :] + stats[4 * p + 3, eight, :]
            both = jnp.concatenate([both] * 16, axis=0).T
            mean = both[:, 0:1] / width
            variance = both[:, 1:2] / width - mean * mean
            normed = (share[at, :] - mean) * lax.rsqrt(variance + epsilon) * gain[...]
            outv[at, :] = normed.astype(BF16)
            writes.append(pltpu.make_async_copy(outv.at[at], out_hbm.at[at], out_sem.at[n]))
            writes[-1].start()

    with jax.named_scope("relay12"):
        relay(1)
        relay(2)
        prepare(0, 1, 2)
    with jax.named_scope("relay03"):
        relay(0)
        relay(3)
        prepare(1, 0, 3)
    with jax.named_scope("settle12"):
        settle(0, 1, 2)
    with jax.named_scope("settle03"):
        settle(1, 0, 3)
    with jax.named_scope("finish12"):
        finish(0, 1, 2)
        into.sent()
        outof.sent()
        for ref, name in (
            (toks.at[pl.ds(0, 3)], "tok"), (part.at[pl.ds(0, 3)], "sum"), (kv.at[pl.ds(0, 2 * WINDOW)], "kv"),
            (chan.at[pl.ds(0, 2 * RIM)], "ch"), (stats.at[pl.ds(0, 3)], "told0"), (stats.at[pl.ds(0, 3)], "told1"),
        ):
            waiting(ref, "send", name)
    with jax.named_scope("finish03"):
        finish(1, 0, 3)
        for write in writes:
            write.wait()
    assert len(groups) == SEMAPHORES


SEMAPHORES = 67


def local(tokens, w_query, w_key, w_value, w_pool_in, sink, w_pool, pool_scale, w_out_attn, w_out_pool, out_gain):
    rows, feats = tokens.shape
    hbm = pl.BlockSpec(memory_space=pltpu.HBM)
    lanes_in = 640
    lanes_out = 512
    model = feats * NY
    return pl.pallas_call(
        kernel,
        out_shape=jax.ShapeDtypeStruct((rows, feats), BF16),
        in_specs=[hbm] * 11,
        out_specs=hbm,
        scratch_shapes=[
            pltpu.VMEM((NY, rows, feats), BF16),
            pltpu.VMEM((NX * NC * NZ, 16, lanes_in), BF16),
            pltpu.VMEM((NX * NC * NZ, 16, lanes_out), BF16),
            pltpu.VMEM((model, lanes_in), BF16),
            pltpu.VMEM((model, lanes_out), BF16),
            pltpu.VMEM((rows, 256), BF16),
            pltpu.VMEM((rows + 2 * WINDOW, 128), BF16),
            pltpu.VMEM((rows + 2 * RIM, 256), BF16),
            pltpu.VMEM((rows, lanes_out), BF16),
            pltpu.VMEM((NY, rows, feats), BF16),
            pltpu.VMEM((rows, feats), BF16),
            pltpu.VMEM((rows, feats), BF16),
            pltpu.VMEM((rows, feats), BF16),
            pltpu.VMEM((rows, feats), BF16),
            pltpu.VMEM((rows, feats), F32),
            pltpu.VMEM((2 * NY, 16, 128), F32),
            pltpu.VMEM((rows, model), BF16),
            pltpu.VMEM((rows, lanes_in), F32),
            pltpu.VMEM((16, 64), BF16),
            pltpu.VMEM((16, 64), BF16),
            pltpu.VMEM((1, 4), F32),
            pltpu.VMEM((1, 256, 256), BF16),
            pltpu.VMEM((1, 256), F32),
            pltpu.VMEM((1, 512), F32),
            pltpu.VMEM((rows, feats), BF16),
            pltpu.SemaphoreType.DMA((11,)),
            pltpu.SemaphoreType.DMA((4,)),
            pltpu.SemaphoreType.DMA((SEMAPHORES,)),
        ],
        compiler_params=pltpu.CompilerParams(
            collective_id=0, has_side_effects=True
        ),
    )(
        tokens, w_query, w_key, w_value, w_pool_in, sink.reshape(1, -1), w_pool, pool_scale.reshape(1, -1),
        w_out_attn.T, w_out_pool.T, out_gain.reshape(1, -1),
    )


def solution(mesh):
    finer = Mesh(mesh.devices.reshape(NZ, NX, NC, NY), (*SP, "tp"))
    return jax.shard_map(
        local,
        mesh=finer,
        in_specs=(
            P(SP, "tp"), P(SP, "tp"), P(SP, "tp"), P(SP, "tp"), P(SP, "tp"), P("tp"),
            P("tp", None, None), P("tp"), P("tp", SP), P("tp", SP), P("tp"),
        ),
        out_specs=P(SP, "tp"),
        check_vma=False,
    )
```

```python
import jax
import jax.numpy as jnp
from jax import lax
from jax.experimental import pallas as pl
from jax.experimental.pallas import tpu as pltpu
from jax.sharding import Mesh
from jax.sharding import PartitionSpec as P

HEAD_DIM = 64
WINDOW = 128
RIM = 16
SP = ("sp_0", "sp_1", "sp_2")
MESH = pl.DeviceIdType.MESH
NZ, NX, NC, NY = 16, 4, 2, 4

epsilon = 1e-05
masked_score = -1e30

OWN, NEAR, REST = 3, (0, 7), (7, 16)
FIRST, SECOND, MIDDLE, FAR = ((1, 4), (4, 6)), ((0, 1), (6, 7)), ((7, 10), (13, 16)), ((10, 12), (12, 13))
NT = (((1,), (1,)), ((), ()))
TN = (((0,), (0,)), ((), ()))
BF16, F32 = jnp.bfloat16, jnp.float32


def kernel(
    tok_hbm, wq_hbm, wk_hbm, wv_hbm, wc_hbm, sink_hbm, wpool_hbm, scale_hbm, woa_hbm, wop_hbm, gain_hbm,
    out_hbm,
    toks, win, wout, win_abs, wout_abs, query, kv, chan, hid, part, comb, relayed, from_prev, from_next,
    share, stats, turned_toks, acc, wk, wv, sink, wpool, scale, gain, outv, local_sem, out_sem, sems,
):
    z, x, c, y = (lax.axis_index(a) for a in (*SP, "tp"))
    rows, feats = toks.shape[1], toks.shape[2]
    seq_len = rows * NZ * NX * NC
    place = (z * NX + x) * NC + c
    offset = place * rows
    total_places = NZ * NX * NC

    def dev_z(d):
        return {"sp_0": lax.rem(z + (d + NZ), NZ)}

    def dev_x(d):
        return {"sp_1": lax.rem(x + (d + NX), NX)}

    def dev_y(d):
        return {"tp": lax.rem(y + (d + NY), NY)}

    dev_c = {"sp_2": 1 - c}

    def dev_sp(d):
        s = lax.rem(place + (d + total_places), total_places)
        return {
            "sp_0": lax.div(s, NX * NC),
            "sp_1": lax.rem(lax.div(s, NC), NX),
            "sp_2": lax.rem(s, NC),
        }

    peers = [dev_z(d) for d in (3, -3, 2, -2, 1, -1)]
    peers += [dev_y(2), dev_sp(1), dev_sp(-1), dev_x(1), dev_x(-1), dev_y(1), dev_y(-1), dev_c]
    mine_in, mine_out = win.at[OWN], wout.at[OWN]
    pairs = (
        (wk_hbm, wk), (wv_hbm, wv), (wq_hbm, mine_in.at[:, pl.ds(0, 256)]), (wc_hbm, mine_in.at[:, pl.ds(384, 256)]),
        (woa_hbm, mine_out.at[:, pl.ds(0, 256)]), (wop_hbm, mine_out.at[:, pl.ds(256, 256)]), (tok_hbm, toks.at[0]),
        (wpool_hbm, wpool), (scale_hbm, scale), (gain_hbm, gain), (sink_hbm, sink),
    )
    loads = [pltpu.make_async_copy(a, b, local_sem.at[k]) for k, (a, b) in enumerate(pairs)]
    for load in loads:
        load.start()

    barrier = pltpu.get_barrier_semaphore()
    for peer in peers:
        pl.semaphore_signal(barrier, inc=1, device_id=peer, device_id_type=MESH)

    with jax.named_scope("entry"):
        loads[0].wait()
        loads[1].wait()
        win[OWN, :, 256:384] = jnp.concatenate([wk[...], wv[...]], axis=1)
        for load in loads[2:6]:
            load.wait()
        pl.semaphore_wait(barrier, len(peers))

    groups = {}

    def message(src, dst, device, sent, got):
        for key in (("send", sent), ("recv", got)):
            groups.setdefault(key, len(groups))
        return pltpu.make_async_remote_copy(
            src_ref=src, dst_ref=dst, send_sem=sems.at[groups["send", sent]], recv_sem=sems.at[groups["recv", got]],
            device_id=device, device_id_type=MESH,
        )

    def waiting(ref, kind, name):
        sem = sems.at[groups[kind, name]]
        copy = pltpu.make_async_remote_copy(
            src_ref=ref, dst_ref=ref, send_sem=sem, recv_sem=sem, device_id=dev_c, device_id_type=MESH
        )
        if kind == "send":
            copy.wait_send()
        else:
            copy.wait_recv()

    class Gather:
        def __init__(self, w, name):
            self.w, self.name = w, name

        def at(self, r, k, lo, hi):
            return self.w.at[pl.ds((r * NC + k) * NZ + lo, hi - lo)]

        def send(self, src, dst, device, got):
            message(src, dst, device, self.name, self.name + got).start()

        def wait(self, slots, got):
            waiting(self.w.at[pl.ds(0, slots)], "recv", self.name + got)

        def pass_on(self, src, dst, d, got):
            self.send(self.at(0, 0, src, src + 1), self.at(0, 0, dst, dst + 1), dev_z(d), got)

        def near(self):
            for d in (1, -1, 2, -2, 3, -3):
                self.pass_on(OWN, (3 - d) % NZ, d, {3: "m3", -3: "p3"}.get(d, "n1"))

        def middle(self):
            self.wait(1, "m3")
            for e in (3, 2, 1):
                self.pass_on(0, 16 - e, e, "m6" if e == 3 else "mid")
            self.wait(1, "p3")
            for e in (3, 2, 1):
                self.pass_on(6, 6 + e, -e, "p6" if e == 3 else "mid")

        def far(self):
            self.wait(1, "m6")
            self.pass_on(13, 11, 2, "far")
            self.pass_on(13, 12, 1, "far")
            self.wait(1, "p6")
            self.pass_on(9, 10, -1, "far")

        def along_x(self, stage):
            up, down = stage
            others = "o%d" % (stage in (MIDDLE, FAR))
            self.send(self.at(0, 0, *up), self.at(3, 0, *up), dev_x(1), "x%d" % up[0])
            self.send(self.at(0, 0, *down), self.at(1, 0, *down), dev_x(-1), "x%d" % down[0])
            self.send(self.at(0, 0, *down), self.at(3, 0, *down), dev_x(1), others)
            self.send(self.at(0, 0, *up), self.at(1, 0, *up), dev_x(-1), others)

        def relay_x(self, stage):
            part = "rest" if stage in (MIDDLE, FAR) else "near"
            for r, d, span in ((3, 1, stage[0]), (1, -1, stage[1])):
                self.wait(span[1] - span[0], "x%d" % span[0])
                self.send(self.at(r, 0, *span), self.at(2, 0, *span), dev_x(d), "x2" + part)

        def across(self, r, span):
            part = "near" if span == NEAR else "rest"
            self.send(self.at(r, 0, *span), self.at(r, 1, *span), dev_c, "c" + part)

        def first(self):
            self.wait(4, "n1")
            self.along_x(FIRST)

        def second(self):
            self.along_x(SECOND)
            self.across(0, NEAR)

        def third(self):
            self.wait(4, "mid")
            self.along_x(MIDDLE)

        def fourth(self):
            self.wait(3, "far")
            self.along_x(FAR)
            self.across(0, REST)

        def others_near(self):
            self.wait(7, "o0")
            self.across(3, NEAR)
            self.across(1, NEAR)

        def others_rest(self):
            self.wait(9, "o1")
            self.across(3, REST)
            self.across(1, REST)

        def last_near(self):
            self.wait(7, "x2near")
            self.across(2, NEAR)

        def last_rest(self):
            self.wait(9, "x2rest")
            self.across(2, REST)

        def in_order(self, dest, span, turned):
            w = self.w
            self.wait(NX * (span[1] - span[0]), "cnear" if span == NEAR else "crest")

            def one(p, carry):
                base = (lax.rem(z + p + (NZ - OWN), NZ) if turned else p) * (NX * NC * 16)
                for r in range(NX):
                    for k in range(NC):
                        at = base + lax.rem(x + r, NX) * (NC * 16) + lax.rem(c + k, NC) * 16
                        dest[pl.ds(pl.multiple_of(at, 16), 16), :] = w[(r * NC + k) * NZ + p]
                return carry

            lax.fori_loop(*span, one, 0)

        def sent(self):
            waiting(self.w.at[pl.ds(0, 127)], "send", self.name)

    into = Gather(win, "in")
    outof = Gather(wout, "out")

    def chunk(b):
        return pl.ds(b * WINDOW, WINDOW)

    def tokens_to(slot, b, src, d, got):
        message(toks.at[src, chunk(b)], toks.at[slot, chunk(b)], dev_y(d), "tok", got).start()

    def tokens_relay(b):
        waiting(toks.at[0, chunk(0)], "recv", "tok%d" % b)
        if b < 2:
            tokens_to(2, b, 3, 1, "tok")
        else:
            tokens_to(2, b, 1, -1, "tok")

    with jax.named_scope("near"):
        into.near()
        loads[6].wait()
        for b in (0, 1):
            tokens_to(3, b, 0, 1, "tok%d" % b)
            tokens_to(1, b + 2, 0, -1, "tok%d" % (b + 2))
        for b in (0, 1):
            tokens_to(3, b + 2, 0, 1, "tok")
            tokens_to(1, b, 0, -1, "tok")
    with jax.named_scope("in_first"):
        into.first()
    with jax.named_scope("in_middle"):
        into.middle()
        outof.near()
        for load in loads[7:]:
            load.wait()
    with jax.named_scope("in_second"):
        into.second()
    with jax.named_scope("tok_relay_a"):
        tokens_relay(0)
        tokens_relay(2)
    with jax.named_scope("in_relay_first"):
        into.relay_x(FIRST)
    with jax.named_scope("in_far"):
        into.far()
    with jax.named_scope("in_third"):
        into.third()
    with jax.named_scope("tok_relay_b"):
        tokens_relay(1)
        tokens_relay(3)
    with jax.named_scope("in_relay_second"):
        into.relay_x(SECOND)
    with jax.named_scope("out_middle"):
        outof.middle()
    with jax.named_scope("in_others_near"):
        into.others_near()
    with jax.named_scope("in_fourth"):
        into.fourth()
    with jax.named_scope("in_relay_third"):
        into.relay_x(MIDDLE)
    with jax.named_scope("out_first"):
        outof.first()
    with jax.named_scope("in_last_near"):
        into.last_near()
    with jax.named_scope("out_far"):
        outof.far()
    with jax.named_scope("in_relay_fourth"):
        into.relay_x(FAR)
    with jax.named_scope("out_second"):
        outof.second()
    with jax.named_scope("in_others_rest"):
        into.others_rest()
    with jax.named_scope("out_third"):
        outof.third()
    with jax.named_scope("in_order_near"):
        into.in_order(win_abs, NEAR, False)
    with jax.named_scope("out_fourth"):
        outof.fourth()
    with jax.named_scope("tok_done"):
        waiting(toks.at[pl.ds(0, 2)], "recv", "tok")
        for p in range(NZ):
            at = lax.rem(z + (p + NZ - OWN), NZ)
            per = feats // 128
            r = lax.rem(lax.div(at, per) + (NY - y), NY)
            cols = pl.ds(pl.multiple_of(lax.rem(at, per) * 128, 128), 128)
            turned_toks[:, p * 128 : (p + 1) * 128] = toks[r, :, cols]

    with jax.named_scope("out_relay_first"):
        outof.relay_x(FIRST)
    with jax.named_scope("in_last_rest"):
        into.last_rest()
    with jax.named_scope("out_relay_second"):
        outof.relay_x(SECOND)
    parts = ((256, 384), (384, 640), (0, 256))
    with jax.named_scope("project_near"):
        depth = slice(NEAR[0] * 128, NEAR[1] * 128)
        for lo, hi in parts:
            acc[:, lo:hi] = jnp.dot(turned_toks[:, depth], win_abs[depth, lo:hi], preferred_element_type=F32)
    with jax.named_scope("out_relay_third"):
        outof.relay_x(MIDDLE)
        outof.others_near()
    with jax.named_scope("in_order_rest"):
        into.in_order(win_abs, REST, False)

    with jax.named_scope("out_relay_fourth"):
        outof.relay_x(FAR)
        outof.others_rest()

    def project(lo, hi):
        depth = slice(REST[0] * 128, REST[1] * 128)
        return acc[:, lo:hi] + jnp.dot(turned_toks[:, depth], win_abs[depth, lo:hi], preferred_element_type=F32)

    own_kv, own_ch = (kv, WINDOW, "kv"), (chan, RIM, "ch")

    def to_neighbours(ref, size, name):
        message(ref.at[pl.ds(rows, size)], ref.at[pl.ds(0, size)], dev_sp(1), name, name).start()
        message(ref.at[pl.ds(size, size)], ref.at[pl.ds(size + rows, size)], dev_sp(-1), name, name).start()

    with jax.named_scope("project"):
        kv[pl.ds(WINDOW, rows), :] = project(256, 384).astype(BF16)
        chan[pl.ds(RIM, rows), :] = project(384, 640).astype(BF16)
        query[...] = (project(0, 256) * HEAD_DIM ** (-0.5)).astype(BF16)
        to_neighbours(*own_kv)
        to_neighbours(*own_ch)

    with jax.named_scope("out_last_near"):
        outof.last_near()

    half = lax.shift_left(jnp.int32(1), y.astype(jnp.int32))
    sinks = jnp.concatenate([jnp.broadcast_to(sink[0:1, h : h + 1], (1, WINDOW)) for h in range(4)], axis=1)

    def attend(n):
        first = offset + n * WINDOW
        band = kv[pl.ds(n * WINDOW, 3 * WINDOW), :]
        keys, values = band[:, :HEAD_DIM], band[:, HEAD_DIM:]
        block = query[n * WINDOW : (n + 1) * WINDOW, :]
        stacked = jnp.concatenate([block[:, h * HEAD_DIM : (h + 1) * HEAD_DIM] for h in range(4)], axis=0)
        scores = lax.dot_general(keys, stacked, NT, preferred_element_type=F32)
        j = lax.broadcasted_iota(jnp.int32, (WINDOW, 4 * WINDOW), 0)
        i = lax.rem(lax.broadcasted_iota(jnp.int32, (WINDOW, 4 * WINDOW), 1), WINDOW)
        before = jnp.where((j >= i) & (first > 0), scores[:WINDOW], masked_score)
        here = scores[WINDOW : 2 * WINDOW]
        after = jnp.where((j <= i) & (first + WINDOW < seq_len), scores[2 * WINDOW :], masked_score)
        top = jnp.max(jnp.maximum(jnp.maximum(before, here), after), axis=0, keepdims=True)
        top = jnp.maximum(top, sinks)
        before, here, after = jnp.exp(before - top), jnp.exp(here - top), jnp.exp(after - top)
        total = jnp.sum(before + here + after, axis=0, keepdims=True) + jnp.exp(sinks - top)
        inverse = 1.0 / total
        probs = jnp.concatenate([(r * inverse).astype(BF16) for r in (before, here, after)], axis=0)
        out = lax.dot_general(values, probs, TN, preferred_element_type=F32)
        out = jnp.concatenate([out[:, h * WINDOW : (h + 1) * WINDOW] for h in range(4)], axis=0)
        hid[n * WINDOW : (n + 1) * WINDOW, 0:256] = out.T.astype(BF16)

    def pool(n):
        first = offset + n * WINDOW
        i = lax.broadcasted_iota(jnp.int32, (WINDOW, WINDOW + 2 * RIM), 0)
        j = lax.broadcasted_iota(jnp.int32, (WINDOW, WINDOW + 2 * RIM), 1) - RIM
        pos = first + j
        member = (j >= i - half) & (j < i + half) & (pos >= 0) & (pos < seq_len)
        member = jnp.where(member, 1.0, 0.0).astype(BF16)
        sums = jnp.dot(member, chan[pl.ds(n * WINDOW, WINDOW + 2 * RIM), :], preferred_element_type=F32)
        t = first + lax.broadcasted_iota(jnp.int32, (WINDOW, 1), 0)
        count = (jnp.minimum(t + half, seq_len) - jnp.maximum(t - half, 0)).astype(F32)
        spread = (sums / count - chan[pl.ds(n * WINDOW + RIM, WINDOW), :].astype(F32)).astype(BF16)
        pooled = jnp.dot(spread, wpool[0], preferred_element_type=F32) * scale[...]
        hid[n * WINDOW : (n + 1) * WINDOW, 256:512] = pooled.astype(BF16)

    def mixers(*which):
        for n in which:
            pool(n)
            attend(n)

    def partials(p, first, second):
        both = jnp.concatenate([hid[chunk(first), :], hid[chunk(second), :]], axis=0)

        def terms(d):
            cols = pl.ds(pl.multiple_of(lax.rem(y + d, NY) * feats, feats), feats)
            out = lax.dot_general(both, wout_abs[cols, :], NT, preferred_element_type=F32).astype(BF16)
            part[d, chunk(first), :] = out[:WINDOW]
            part[d, chunk(second), :] = out[WINDOW:]

        terms(2)
        for n in (first, second):
            target = dev_y(1 if n < 2 else -1)
            message(part.at[2, chunk(n)], relayed.at[chunk(n)], target, "sum", "via%d" % n).start()
        for d in (3, 1, 0):
            terms(d)
        for n in (first, second):
            if n < 2:
                message(part.at[3, chunk(n)], from_next.at[chunk(n)], dev_y(-1), "sum", "one%d" % p).start()
            else:
                message(part.at[1, chunk(n)], from_prev.at[chunk(n)], dev_y(1), "sum", "one%d" % p).start()

    def relay(n):
        at = chunk(n)
        waiting(relayed.at[at], "recv", "via%d" % n)
        mine = part[1 if n < 2 else 3, at, :]
        comb[at, :] = (mine.astype(F32) + relayed[at, :].astype(F32)).astype(BF16)
        got = "sum%d" % (n in (0, 3))
        if n < 2:
            message(comb.at[at], from_prev.at[at], dev_y(1), "sum", got).start()
        else:
            message(comb.at[at], from_next.at[at], dev_y(-1), "sum", got).start()

    with jax.named_scope("mix1"):
        mixers(1)
    with jax.named_scope("out_last_rest"):
        outof.last_rest()
    with jax.named_scope("mix2"):
        mixers(2)
    with jax.named_scope("out_order_near"):
        outof.in_order(wout_abs, NEAR, True)
    with jax.named_scope("out_order_rest"):
        outof.in_order(wout_abs, REST, True)
    with jax.named_scope("part12"):
        partials(0, 1, 2)
    with jax.named_scope("halo"):
        waiting(kv.at[pl.ds(0, 2 * WINDOW)], "recv", "kv")
        waiting(chan.at[pl.ds(0, 2 * RIM)], "recv", "ch")
    with jax.named_scope("mix03"):
        mixers(0, 3)
    with jax.named_scope("part03"):
        partials(1, 0, 3)
    lane = lax.broadcasted_iota(jnp.int32, (WINDOW, 128), 1)

    def prepare(p, first, second):
        waiting(from_prev.at[pl.ds(0, 2 * WINDOW)], "recv", "one%d" % p)
        for n in (first, second):
            at = chunk(n)
            single = (from_next if n < 2 else from_prev)[at, :]
            share[at, :] = part[0, at, :].astype(F32) + single.astype(F32)

    def settle(p, first, second):
        waiting(from_prev.at[pl.ds(0, 2 * WINDOW)], "recv", "sum%d" % p)
        for k, n in enumerate((first, second)):
            at = chunk(n)
            mix = share[at, :] + (from_prev if n < 2 else from_next)[at, :].astype(F32)
            share[at, :] = mix
            one = jnp.sum(mix, axis=1, keepdims=True)
            two = jnp.sum(mix * mix, axis=1, keepdims=True)
            both = jnp.where(lane == 0, one, jnp.where(lane == 1, two, 0.0))
            stats[4 * p, k * 8 : k * 8 + 8, :] = both.T[0:8]
        for d, slot in ((2, 2), (1, 3), (-1, 1)):
            message(stats.at[4 * p], stats.at[4 * p + slot], dev_y(d), "told%d" % p, "told%d" % p).start()

    width = feats * NY
    writes = []

    def finish(p, first, second):
        waiting(stats.at[pl.ds(0, 3)], "recv", "told%d" % p)
        for k, n in enumerate((first, second)):
            eight = slice(k * 8, k * 8 + 8)
            both = stats[4 * p, eight, :] + stats[4 * p + 1, eight, :]
            both = both + stats[4 * p + 2, eight, :] + stats[4 * p + 3, eight, :]
            both = jnp.concatenate([both] * 16, axis=0).T
            mean = both[:, 0:1] / width
            variance = both[:, 1:2] / width - mean * mean
            rise = lax.rsqrt(variance + epsilon)
            for m in range(2):
                top, size = m * (WINDOW // 2), WINDOW // 2
                at = pl.ds(n * WINDOW + top, size)
                normed = (share[at, :] - mean[top : top + size]) * rise[top : top + size] * gain[...]
                outv[at, :] = normed.astype(BF16)
                writes.append(pltpu.make_async_copy(outv.at[at], out_hbm.at[at], out_sem.at[2 * n + m]))
                writes[-1].start()

    with jax.named_scope("relay12"):
        relay(1)
        relay(2)
        prepare(0, 1, 2)
    with jax.named_scope("relay03"):
        relay(0)
        relay(3)
        prepare(1, 0, 3)
    with jax.named_scope("settle12"):
        settle(0, 1, 2)
    with jax.named_scope("settle03"):
        settle(1, 0, 3)
    with jax.named_scope("finish12"):
        finish(0, 1, 2)
        into.sent()
        outof.sent()
        for ref, name in (
            (toks.at[pl.ds(0, 3)], "tok"), (part.at[pl.ds(0, 3)], "sum"), (kv.at[pl.ds(0, 2 * WINDOW)], "kv"),
            (chan.at[pl.ds(0, 2 * RIM)], "ch"), (stats.at[pl.ds(0, 3)], "told0"), (stats.at[pl.ds(0, 3)], "told1"),
        ):
            waiting(ref, "send", name)
    with jax.named_scope("finish03"):
        finish(1, 0, 3)
        for write in writes:
            write.wait()
    assert len(groups) == SEMAPHORES


SEMAPHORES = 67


def local(tokens, w_query, w_key, w_value, w_pool_in, sink, w_pool, pool_scale, w_out_attn, w_out_pool, out_gain):
    rows, feats = tokens.shape
    hbm = pl.BlockSpec(memory_space=pltpu.HBM)
    lanes_in = 640
    lanes_out = 512
    model = feats * NY
    return pl.pallas_call(
        kernel,
        out_shape=jax.ShapeDtypeStruct((rows, feats), BF16),
        in_specs=[hbm] * 11,
        out_specs=hbm,
        scratch_shapes=[
            pltpu.VMEM((NY, rows, feats), BF16),
            pltpu.VMEM((NX * NC * NZ, 16, lanes_in), BF16),
            pltpu.VMEM((NX * NC * NZ, 16, lanes_out), BF16),
            pltpu.VMEM((model, lanes_in), BF16),
            pltpu.VMEM((model, lanes_out), BF16),
            pltpu.VMEM((rows, 256), BF16),
            pltpu.VMEM((rows + 2 * WINDOW, 128), BF16),
            pltpu.VMEM((rows + 2 * RIM, 256), BF16),
            pltpu.VMEM((rows, lanes_out), BF16),
            pltpu.VMEM((NY, rows, feats), BF16),
            pltpu.VMEM((rows, feats), BF16),
            pltpu.VMEM((rows, feats), BF16),
            pltpu.VMEM((rows, feats), BF16),
            pltpu.VMEM((rows, feats), BF16),
            pltpu.VMEM((rows, feats), F32),
            pltpu.VMEM((2 * NY, 16, 128), F32),
            pltpu.VMEM((rows, model), BF16),
            pltpu.VMEM((rows, lanes_in), F32),
            pltpu.VMEM((16, 64), BF16),
            pltpu.VMEM((16, 64), BF16),
            pltpu.VMEM((1, 4), F32),
            pltpu.VMEM((1, 256, 256), BF16),
            pltpu.VMEM((1, 256), F32),
            pltpu.VMEM((1, 512), F32),
            pltpu.VMEM((rows, feats), BF16),
            pltpu.SemaphoreType.DMA((11,)),
            pltpu.SemaphoreType.DMA((8,)),
            pltpu.SemaphoreType.DMA((SEMAPHORES,)),
        ],
        compiler_params=pltpu.CompilerParams(
            collective_id=0, has_side_effects=True
        ),
    )(
        tokens, w_query, w_key, w_value, w_pool_in, sink.reshape(1, -1), w_pool, pool_scale.reshape(1, -1),
        w_out_attn.T, w_out_pool.T, out_gain.reshape(1, -1),
    )


def solution(mesh):
    finer = Mesh(mesh.devices.reshape(NZ, NX, NC, NY), (*SP, "tp"))
    return jax.shard_map(
        local,
        mesh=finer,
        in_specs=(
            P(SP, "tp"), P(SP, "tp"), P(SP, "tp"), P(SP, "tp"), P(SP, "tp"), P("tp"),
            P("tp", None, None), P("tp"), P("tp", SP), P("tp", SP), P("tp"),
        ),
        out_specs=P(SP, "tp"),
        check_vma=False,
    )
```
